512 devices in a mesh: sp: 256 (over z, y, x), tp: 2 (over core).
Axes of the slice: x: 4, y: 8, z: 8, core: 2. Of those that a mesh axis runs over, the one named last changes fastest.
Arguments:
- features: bfloat16 [65536, 1024], P('sp', 'tp'), may hold values from -6 to 6
- lambda_real: float32 [64, 64], P('tp'), may hold values from -4 to 0, as said below
- lambda_imag: float32 [64, 64], P('tp'), may hold values from 0.5 to 201.06177
- log_step: float32 [64], P('tp'), may hold values from -5 to -2
- input_real: float32 [64, 64, 16], P('tp'), may hold values from -0.5 to 0.5
- input_imag: float32 [64, 64, 16], P('tp'), may hold values from -0.5 to 0.5
- real_output: float32 [64, 16, 64], P('tp'), may hold values from -0.75 to 0.75
- imaginary_output: float32 [64, 16, 64], P('tp'), may hold values from -0.75 to 0.75
- skip_gain: float32 [1024], P('tp'), may hold values from -4 to 4
- value_weight: bfloat16 [1024, 2048], P('tp'), may hold values from -0.1875 to 0.1875
- gate_weight: bfloat16 [1024, 2048], P('tp'), may hold values from -0.1875 to 0.1875
- value_bias: float32 [2048], replicated, may hold values from -3 to 3
- gate_bias: float32 [2048], replicated, may hold values from -3 to 3
Outputs:
- mixed_output: bfloat16 [65536, 2048], P(('sp', 'tp'))
The draws below stay inside these ranges and needn't reach their ends.
Inputs may be any that keep to these rules, and one draw needn't show every extreme that they name: `lambda_real`: negative.
All inputs are finite; a program needn't handle non-finite values.
Results may differ from the reference program's by a relative error of at most 0.03.
Values may be sent and summed in bfloat16 or wider, within the bound.
A program may use at most 128 MiB of HBM per device.

```python
import math
import jax
import jax.numpy as jnp
from jax import lax

D = 2048
CHANNELS = 1024
GROUP = 16
STATE = 64
TOK_SP = 256
GROUPS = 64
LENGTH = 65536
N_TP = 2


def group_rates(key):
    base_key = jax.random.fold_in(key, 91)
    key_flag, key_step, key_rate = jax.random.split(base_key, 3)
    fast_share = 5
    fast_flag = jax.random.randint(key_flag, (GROUPS,), 0, 10) < fast_share
    log_step = jax.random.uniform(key_step, (GROUPS,), jnp.float32, math.log(0.01), math.log(0.1))
    step_size = jnp.exp(log_step)[:, None]
    rate_draw = jax.random.uniform(key_rate, (GROUPS, STATE), jnp.float32, 0.0, 1.0)
    fast_rate = (0.01 + 0.023 * rate_draw) / step_size
    slow_rate = (0.3 + 1.7 * rate_draw) / (LENGTH * step_size)
    lambda_real = -jnp.where(fast_flag[:, None], fast_rate, slow_rate)
    return (lambda_real.astype(jnp.float32), log_step.astype(jnp.float32))


def draw_lambda_real(key, part):
    return group_rates(key)[0]


def draw_log_step(key, part):
    return group_rates(key)[1]


def block_levels(key, dims, cuts, low, top_value):
    loudness = 1.0
    for dim, blocks in cuts:
        draws = jax.random.uniform(jax.random.fold_in(jax.random.fold_in(key, 6), dim), (blocks,), jnp.float32, low / len(cuts), top_value / len(cuts))
        loudness = loudness * jnp.repeat(jnp.exp(draws), dims[dim] // blocks).reshape((-1,) + (1,) * (len(dims) - 1 - dim))
    return loudness


def normal_values(own_key, extent, width, bound, pieces=(), held_as=jnp.bfloat16):
    values = jax.random.normal(own_key, extent, jnp.float32) * width
    if len(pieces) > 0:
        values = block_levels(own_key, extent, pieces, -0.22, 0.18) * values
    return jnp.clip(values, min=-bound, max=bound).astype(held_as)


def setup_inputs(seed: int = 0) -> dict:
    splits = jax.random.split(jax.random.key(seed), 14)
    return {
        "features": normal_values(splits[0], (LENGTH, CHANNELS), 1.0, 6.0, ((0, 256), (1, 2))),
        "lambda_real": draw_lambda_real(jax.random.fold_in(splits[13], 71), 0),
        "lambda_imag": jnp.clip(0.5 + 200.56177 * jax.random.uniform(splits[2], (GROUPS, STATE), jnp.float32) ** block_levels(splits[2], (GROUPS, STATE), ((0, 2),), -0.2, 0.2), 0.5, 201.06177),
        "log_step": draw_log_step(jax.random.fold_in(splits[13], 71), 0),
        "input_real": normal_values(splits[4], (GROUPS, STATE, GROUP), (max(4, LENGTH // 512)) ** -0.5, 0.5, ((0, 2),), jnp.float32),
        "input_imag": normal_values(splits[5], (GROUPS, STATE, GROUP), (max(4, LENGTH // 512)) ** -0.5, 0.5, ((0, 2),), jnp.float32),
        "real_output": normal_values(splits[6], (GROUPS, GROUP, STATE), STATE ** -0.5, 0.75, ((0, 2),), jnp.float32),
        "imaginary_output": normal_values(splits[7], (GROUPS, GROUP, STATE), STATE ** -0.5, 0.75, ((0, 2),), jnp.float32),
        "skip_gain": normal_values(splits[8], (CHANNELS,), 1.0, 4.0, ((0, 2),), jnp.float32),
        "value_weight": normal_values(splits[9], (CHANNELS, D), CHANNELS ** -0.5, 0.1875, ((0, 2),)),
        "gate_weight": normal_values(splits[10], (CHANNELS, D), CHANNELS ** -0.5, 0.1875, ((0, 2),)),
        "value_bias": normal_values(splits[11], (D,), 0.5, 3.0, (), jnp.float32),
        "gate_bias": normal_values(splits[12], (D,), 0.5, 3.0, (), jnp.float32),
    }


def discretize(lambda_real, lambda_imag, log_step, input_real, input_imag):
    step_size = jnp.exp(log_step)[:, None]
    magnitude = jnp.exp(lambda_real * step_size)
    phase_arg = lambda_imag * step_size
    trans_re = magnitude * jnp.cos(phase_arg)
    trans_im = magnitude * jnp.sin(phase_arg)
    denominator = lambda_real * lambda_real + lambda_imag * lambda_imag
    num_re = trans_re - 1.0
    num_im = trans_im
    f_re = (num_re * lambda_real + num_im * lambda_imag) / denominator
    f_im = (num_im * lambda_real - num_re * lambda_imag) / denominator
    bar_re = f_re[..., None] * input_real - f_im[..., None] * input_imag
    bar_im = f_re[..., None] * input_imag + f_im[..., None] * input_real
    return step_size, bar_re, bar_im


def powers(lambda_real, lambda_imag, step_size, positions):
    exponent = (jnp.arange(positions, dtype=jnp.int32) + 1).astype(jnp.float32)[:, None, None]
    magnitude = jnp.exp(exponent * lambda_real * step_size)
    phase_arg = exponent * lambda_imag * step_size
    return magnitude * jnp.cos(phase_arg), magnitude * jnp.sin(phase_arg)


def combine(earlier, later):
    a1r, a1i, b1r, b1i = earlier
    a2r, a2i, b2r, b2i = later
    return (a1r * a2r - a1i * a2i, a1r * a2i + a1i * a2r,
            a2r * b1r - a2i * b1i + b2r, a2r * b1i + a2i * b1r + b2i)


def local_states(trans_re, trans_im, bu_re, bu_im):
    a_re = jnp.broadcast_to(trans_re, bu_re.shape)
    a_im = jnp.broadcast_to(trans_im, bu_im.shape)
    result = lax.associative_scan(combine, (a_re, a_im, bu_re, bu_im), axis=0)
    return result[2], result[3]


def reference(features, lambda_real, lambda_imag, log_step, input_real, input_imag, real_output,
              imaginary_output, skip_gain, value_weight, gate_weight, value_bias, gate_bias):
    upper_limit = lax.Precision.HIGHEST
    step_size, bar_re, bar_im = discretize(lambda_real, lambda_imag, log_step, input_real, input_imag)
    pw_re, pw_im = powers(lambda_real, lambda_imag, step_size, TOK_SP)
    blocks = features.reshape(LENGTH // TOK_SP, TOK_SP, CHANNELS)
    slice_width = CHANNELS // N_TP

    def partials(activated, weight):
        total = jnp.zeros((TOK_SP, D), jnp.float32)
        for index in range(N_TP):
            left = activated[:, index * slice_width:(index + 1) * slice_width]
            right = weight[index * slice_width:(index + 1) * slice_width]
            rounded = lax.optimization_barrier(jnp.dot(left, right, preferred_element_type=jnp.float32).astype(jnp.bfloat16))
            total = total + rounded.astype(jnp.float32)
        return total

    def advance(carried, rows_per_block):
        h_re, h_im = carried
        widened = rows_per_block.astype(jnp.float32)
        grouped = widened.reshape(TOK_SP, GROUPS, GROUP)
        bu_re = jnp.einsum('sgc,gpc->sgp', grouped, bar_re, precision=upper_limit)
        bu_im = jnp.einsum('sgc,gpc->sgp', grouped, bar_im, precision=upper_limit)
        signal_real, signal_imaginary = local_states(pw_re[0], pw_im[0], bu_re, bu_im)
        signal_real = signal_real + pw_re * h_re - pw_im * h_im
        signal_imaginary = signal_imaginary + pw_re * h_im + pw_im * h_re
        mixer_response = (jnp.einsum('qej,eoj->qeo', signal_real, real_output, precision=upper_limit)
                    - jnp.einsum('qej,eoj->qeo', signal_imaginary, imaginary_output, precision=upper_limit))
        mixer_response = mixer_response.reshape(TOK_SP, CHANNELS) + skip_gain * widened
        activated = jax.nn.gelu(mixer_response).astype(jnp.bfloat16)
        value_sum = partials(activated, value_weight) + value_bias
        gate_sum = partials(activated, gate_weight) + gate_bias
        result = (value_sum * jax.nn.sigmoid(gate_sum)).astype(jnp.bfloat16)
        return (signal_real[-1], signal_imaginary[-1]), result

    start_state = (jnp.zeros((GROUPS, STATE), jnp.float32), jnp.zeros((GROUPS, STATE), jnp.float32))
    _, outputs = lax.scan(advance, start_state, blocks)
    return outputs.reshape(LENGTH, D)
```

```python
import functools

import jax
import jax.numpy as jnp
from jax import lax
from jax.experimental import pallas as pl
from jax.experimental.pallas import tpu as pltpu
from jax.sharding import PartitionSpec as P

MESH = pl.DeviceIdType.MESH
F32 = jnp.float32
BF16 = jnp.bfloat16


def iota(shape, dim):
    return lax.broadcasted_iota(jnp.int32, shape, dim)


def cmul(ar, ai, br, bi):
    return ar * br - ai * bi, ar * bi + ai * br


def nt_dot(left, right):
    return lax.dot_general(left, right, (((1,), (1,)), ((), ())), preferred_element_type=F32)


def split_ring(nsp):
    nx = min(8, nsp)
    ny = min(8, nsp // nx)
    return nsp // (nx * ny), ny, nx


def kernel(ring, ntp, dims, *refs):
    nz, ny, nx = ring
    rows, groups, state, size, width = dims
    (x_h, lr_h, li_h, ls_h, br_h, bi_h, cr_h, ci_h, sk_h, vw_h, gw_h, vb_h, gb_h, out_ref,
     x_v, lr_v, li_v, ls_v, br_v, bi_v, cr_v, ci_v, sk_v, vw_v, gw_v, vb_v, gb_v,
     xp_v, zr_v, zi_v, zcat_v, wcat_v, crm_v, cim_v, resp_v, act_v,
     hx_v, fin_v, a_all_v, tab_x, tab_y, msg_v, recv_x, recv_y, recv_z, h_v, part_v, inbox_v,
     in_sem, send_x, got_x, send_y, got_y, send_z, got_z, psend_sem, precv_sem) = refs
    me = lax.axis_index("sp")
    core = lax.axis_index("tp")
    x, y, z = lax.rem(me, nx), lax.rem(me // nx, ny), me // (nx * ny)
    gpb = 128 // size
    lanes = gpb * state
    blocks = groups // gpb
    chunks = 16
    length = rows // chunks
    own_rows = rows // ntp
    tall, wide = fin_v.shape[0] // 2, fin_v.shape[1]
    fold = lanes // wide

    hbm = (ls_h, lr_h, li_h, x_h, br_h, bi_h, cr_h, ci_h, sk_h, vb_h, gb_h, vw_h, gw_h)
    vmem = (ls_v, lr_v, li_v, x_v, br_v, bi_v, cr_v, ci_v, sk_v, vb_v, gb_v, vw_v, gw_v)
    copies = [pltpu.make_async_copy(s, d, in_sem.at[i]) for i, (s, d) in enumerate(zip(hbm, vmem))]
    for c in copies[:6]:
        c.start()

    barrier = pltpu.get_barrier_semaphore()
    for k in range(1, ntp):
        pl.semaphore_signal(barrier, inc=1, device_id=(me, lax.rem(core + k, ntp)), device_id_type=MESH)

    def peer(at, count, stride, k):
        other = lax.rem(at + k, count)
        return other, (me + (other - at) * stride, core)

    lines = ((x, nx, 1), (y, ny, nx), (z, nz, nx * ny))
    for line in lines:
        for k in range(1, line[1]):
            pl.semaphore_signal(barrier, inc=1, device_id=peer(*line, k)[1], device_id_type=MESH)

    for c in copies[:3]:
        c.wait()
    eye = iota((groups, groups), 0) == iota((groups, groups), 1)
    step = jnp.exp(jnp.sum(jnp.where(eye, ls_v[...], 0.0), axis=1, keepdims=True))
    lam_r, lam_i = lr_v[...], li_v[...]
    mag = jnp.exp(lam_r * step)
    phase = lam_i * step
    t_r, t_i = mag * jnp.cos(phase), mag * jnp.sin(phase)
    den = lam_r * lam_r + lam_i * lam_i
    n_r = t_r - 1.0
    f_r = (n_r * lam_r + t_i * lam_i) / den
    f_i = (t_i * lam_r - n_r * lam_i) / den

    per = 128 // state
    row8, lane8 = iota((gpb, 128), 0), iota((gpb, 128), 1)

    def flat(value, b):
        sub = value[b * gpb:(b + 1) * gpb]
        dup = jnp.concatenate([sub] * per, axis=1)
        return jnp.concatenate(
            [jnp.sum(jnp.where(row8 == per * j + lane8 // state, dup, 0.0), axis=0, keepdims=True)
             for j in range(gpb // per)], axis=1)

    r0, r1 = iota((rows, rows), 0), iota((rows, rows), 1)
    shuffle = jnp.where(r1 == (r0 % chunks) * length + r0 // chunks, 1.0, 0.0).astype(BF16)
    copies[3].wait()
    xp_v[...] = jnp.dot(shuffle, x_v[...], preferred_element_type=F32).astype(BF16)


    c_mask = iota((128, lanes), 0) // size == iota((128, lanes), 1) // state

    def diagonal(tall):
        return jnp.where(c_mask, jnp.concatenate([tall] * gpb, axis=1), 0.0)

    copies[4].wait()
    copies[5].wait()
    for c in copies[6:]:
        c.start()
    crow = iota((chunks, lanes), 0)

    def shift(value, s):
        return jnp.where(crow >= s, pltpu.roll(value, s, 0), 0.0)

    for b in range(blocks):
        xb = xp_v[:, b * 128:(b + 1) * 128]

        def inject(ref):
            mat = diagonal(ref[b * gpb:(b + 1) * gpb].reshape(128, state)).astype(BF16)
            return jnp.dot(xb, mat, preferred_element_type=F32)

        zr_v[b] = inject(br_v)
        zi_v[b] = inject(bi_v)
        a1r, a1i = flat(t_r, b), flat(t_i, b)
        ar, ai = jnp.broadcast_to(a1r, (chunks, lanes)), jnp.broadcast_to(a1i, (chunks, lanes))
        z_r = z_i = None
        for o in range(length):
            here = pl.ds(o * chunks, chunks)
            if o == 0:
                z_r, z_i = zr_v[b, here, :], zi_v[b, here, :]
            else:
                p_r, p_i = cmul(ar, ai, z_r, z_i)
                z_r, z_i = p_r + zr_v[b, here, :], p_i + zi_v[b, here, :]
                zr_v[b, here, :] = z_r
                zi_v[b, here, :] = z_i
        qr, qi = ar, ai
        s = 1
        while s < length:
            qr, qi = cmul(qr, qi, qr, qi)
            s *= 2
        pw_r, pw_i = jnp.ones_like(qr), jnp.zeros_like(qr)
        s = 1
        while s < chunks:
            m_r, m_i = cmul(qr, qi, shift(z_r, s), shift(z_i, s))
            z_r, z_i = z_r + m_r, z_i + m_i
            bit = (crow // s) % 2 == 1
            pw_r, pw_i = cmul(pw_r, pw_i, jnp.where(bit, qr, 1.0), jnp.where(bit, qi, 0.0))
            qr, qi = cmul(qr, qi, qr, qi)
            s *= 2
        hx_v[0, b], hx_v[1, b] = shift(z_r, 1), shift(z_i, 1)
        for ref, val_r, val_i in ((fin_v, z_r[chunks - 1:], z_i[chunks - 1:]), (a_all_v, qr[:1], qi[:1])):
            for u in range(fold):
                at, cols = b * fold + u, slice(u * wide, (u + 1) * wide)
                ref[at:at + 1] = val_r[:, cols]
                ref[tall + at:tall + at + 1] = val_i[:, cols]
        hx_v[2, b], hx_v[3, b] = pw_r, pw_i
    msg_v[0] = fin_v[...].astype(BF16)

    pl.semaphore_wait(barrier, nx - 1 + ny - 1 + nz - 1 + ntp - 1)

    def outgoing(stage, k):
        at = lines[stage][0]
        other, device = peer(*lines[stage], k)
        return pltpu.make_async_remote_copy(
            src_ref=msg_v.at[stage], dst_ref=(recv_x, recv_y, recv_z)[stage].at[at],
            send_sem=(send_x, send_y, send_z)[stage].at[other], recv_sem=(got_x, got_y, got_z)[stage].at[at],
            device_id=device, device_id_type=MESH)

    def incoming(stage, k):
        other, device = peer(*lines[stage], k)
        recv = (recv_x, recv_y, recv_z)[stage].at[other]
        pltpu.make_async_remote_copy(
            src_ref=msg_v.at[stage], dst_ref=recv,
            send_sem=(send_x, send_y, send_z)[stage].at[other], recv_sem=(got_x, got_y, got_z)[stage].at[other],
            device_id=device, device_id_type=MESH).wait_recv()
        got = recv[...].astype(F32)
        return other, got[:tall], got[tall:]

    def near_first(count):
        return sorted(range(1, count), key=lambda k: min(k, count - k))

    for k in reversed(near_first(nx)):
        outgoing(0, k).start()

    def powers(tab, count, a_r, a_i):
        p_r, p_i = jnp.ones((tall, wide), F32), jnp.zeros((tall, wide), F32)
        for i in range(count):
            tab[i] = jnp.zeros((2 * tall, wide), F32)
            tab[count + i, :tall], tab[count + i, tall:] = p_r, p_i
            p_r, p_i = cmul(p_r, p_i, a_r, a_i)
        return p_r, p_i

    ax_r, ax_i = powers(tab_x, nx, a_all_v[:tall], a_all_v[tall:])
    ay_r, ay_i = powers(tab_y, ny, ax_r, ax_i)

    def weight(tab, at, v_r, v_i):
        return cmul(tab[at, :tall], tab[at, tall:], v_r, v_i)

    def collect(stage, tab, own_r, own_i):
        at, count, _ = lines[stage]
        t_r, t_i = weight(tab, count + count - 1 - at, own_r, own_i)
        p_r = p_i = jnp.zeros((tall, wide), F32)
        for k in near_first(count):
            other, v_r, v_i = incoming(stage, k)
            m_r, m_i = weight(tab, count + count - 1 - other, v_r, v_i)
            t_r, t_i = t_r + m_r, t_i + m_i
            m_r, m_i = weight(tab, count + at - 1 - other, v_r, v_i)
            p_r, p_i = p_r + m_r, p_i + m_i
        return t_r, t_i, p_r, p_i

    copies[6].wait()
    copies[7].wait()
    copies[8].wait()
    def respond(b):
        a1r, a1i = flat(t_r, b), flat(t_i, b)
        ar, ai = jnp.broadcast_to(a1r, (chunks, lanes)), jnp.broadcast_to(a1i, (chunks, lanes))
        w_r, w_i = hx_v[0, b], hx_v[1, b]
        p_r, p_i = hx_v[2, b], hx_v[3, b]
        for o in range(length):
            here = pl.ds(o * chunks, chunks)
            w_r, w_i = cmul(ar, ai, w_r, w_i)
            p_r, p_i = cmul(ar, ai, p_r, p_i)
            zcat_v[here, :lanes] = (zr_v[b, here, :] + w_r).astype(BF16)
            zcat_v[here, lanes:] = (zi_v[b, here, :] + w_i).astype(BF16)
            wcat_v[b, here, :lanes] = p_r.astype(BF16)
            wcat_v[b, here, lanes:] = p_i.astype(BF16)
        gains_r, gains_i = [], []
        for g in range(b * gpb, (b + 1) * gpb):
            g_r, g_i = cmul(cr_v[g], ci_v[g], f_r[g:g + 1], f_i[g:g + 1])
            gains_r.append(g_r)
            gains_i.append(g_i)

        m_r = diagonal(jnp.concatenate(gains_r, axis=0))
        m_i = diagonal(jnp.concatenate(gains_i, axis=0))
        crm_v[b], cim_v[b] = m_r, m_i
        mats = jnp.concatenate([m_r.astype(BF16), (-m_i).astype(BF16)], axis=1)
        col = pl.ds(b * 128, 128)
        resp_v[:, col] = nt_dot(zcat_v[...], mats) + sk_v[:, col] * xp_v[:, col].astype(F32)

    half = blocks // 2
    for b in range(half):
        respond(b)
    row_r, row_i, hx_r, hx_i = collect(0, tab_x, fin_v[:tall], fin_v[tall:])
    msg_v[1, :tall], msg_v[1, tall:] = row_r.astype(BF16), row_i.astype(BF16)
    for k in reversed(near_first(ny)):
        outgoing(1, k).start()
    for b in range(half, blocks):
        respond(b)
    plane_r, plane_i, hy_r, hy_i = collect(1, tab_y, row_r, row_i)
    msg_v[2, :tall], msg_v[2, tall:] = plane_r.astype(BF16), plane_i.astype(BF16)

    @pl.loop(z + 1, nz)
    def _(d):
        outgoing(2, d - z).start()

    m_r, m_i = weight(tab_x, nx + x, hy_r, hy_i)
    h_r, h_i = hx_r + m_r, hx_i + m_i
    s_r, s_i = weight(tab_x, nx + x, tab_y[ny + y, :tall], tab_y[ny + y, tall:])

    def gather(k, carry):
        h_r, h_i, p_r, p_i = carry
        _, v_r, v_i = incoming(2, nz - 1 - k)
        m_r, m_i = cmul(p_r, p_i, v_r, v_i)
        return (h_r + m_r, h_i + m_i) + cmul(p_r, p_i, ay_r, ay_i)

    h_r, h_i, _, _ = lax.fori_loop(0, z, gather, (h_r, h_i, s_r, s_i))
    h_v[:tall] = h_r
    h_v[tall:] = h_i

    def flat_h(at, b):
        return jnp.concatenate([h_v[at + b * fold + u:at + b * fold + u + 1] for u in range(fold)], axis=1)

    for b in range(blocks):
        k_r, k_i = cmul(crm_v[b], cim_v[b], flat_h(0, b), flat_h(tall, b))
        mats = jnp.concatenate([k_r.astype(BF16), (-k_i).astype(BF16)], axis=1)
        col = pl.ds(b * 128, 128)
        total = resp_v[:, col] + nt_dot(wcat_v[b], mats)
        act_v[:, col] = jax.nn.gelu(total).astype(BF16)

    back = jnp.where(r1 == (r0 % length) * chunks + r0 // length, 1.0, 0.0).astype(BF16)
    act = jnp.dot(back, act_v[...], preferred_element_type=F32).astype(BF16)

    for c in copies[9:]:
        c.wait()
    piece = inbox_v.shape[-1]
    pieces = width // piece

    def exchange(j, k):
        to = lax.rem(core + k, ntp)
        return pltpu.make_async_remote_copy(
            src_ref=part_v.at[j, to], dst_ref=inbox_v.at[j, k - 1],
            send_sem=psend_sem.at[j, k - 1], recv_sem=precv_sem.at[j, k - 1],
            device_id=(me, to), device_id_type=MESH)

    for j in range(pieces):
        col = pl.ds(j * piece, piece)
        for which, weight in enumerate((vw_v, gw_v)):
            part = jnp.dot(act, weight[:, col], preferred_element_type=F32).astype(BF16)
            for i in range(ntp):
                part_v[j, i, which] = part[i * own_rows:(i + 1) * own_rows]
        for k in range(1, ntp):
            exchange(j, k).start()
    for j in range(pieces):
        col = pl.ds(j * piece, piece)
        for k in range(1, ntp):
            exchange(j, k).wait_recv()
        sums = []
        for which, bias in enumerate((vb_v, gb_v)):
            total = part_v[j, core, which].astype(F32)
            for k in range(1, ntp):
                total = total + inbox_v[j, k - 1, which].astype(F32)
            sums.append(total + bias[:, col])
        out_ref[:, col] = (sums[0] * jax.nn.sigmoid(sums[1])).astype(BF16)
    for j in range(pieces):
        for k in range(1, ntp):
            exchange(j, k).wait_send()

    for stage in range(2):
        for k in range(1, lines[stage][1]):
            outgoing(stage, k).wait_send()

    @pl.loop(z + 1, nz)
    def _(d):
        outgoing(2, d - z).wait_send()


def local(nsp, ntp, features, lambda_real, lambda_imag, log_step, input_real, input_imag, real_output,
          imaginary_output, skip_gain, value_weight, gate_weight, value_bias, gate_bias):
    rows, channels = features.shape
    groups, state = lambda_real.shape
    size = input_real.shape[2]
    input_real, input_imag = jnp.swapaxes(input_real, 1, 2), jnp.swapaxes(input_imag, 1, 2)
    width = value_weight.shape[1]
    gpb = 128 // size
    lanes, blocks, chunks = gpb * state, groups // gpb, 16
    piece = min(512, width)
    ring = nz, ny, nx = split_ring(nsp)
    held = (16, 2 * blocks * lanes // 16)
    args = (features, lambda_real, lambda_imag, log_step[None], input_real, input_imag, real_output,
            imaginary_output, skip_gain[None], value_weight, gate_weight, value_bias[None], gate_bias[None])
    scratch = [pltpu.VMEM(a.shape, a.dtype) for a in args]
    scratch += [
        pltpu.VMEM((rows, channels), BF16),
        pltpu.VMEM((blocks, rows, lanes), F32),
        pltpu.VMEM((blocks, rows, lanes), F32),
        pltpu.VMEM((rows, 2 * lanes), BF16),
        pltpu.VMEM((blocks, rows, 2 * lanes), BF16),
        pltpu.VMEM((blocks, 128, lanes), F32),
        pltpu.VMEM((blocks, 128, lanes), F32),
        pltpu.VMEM((rows, channels), F32),
        pltpu.VMEM((rows, channels), BF16),
        pltpu.VMEM((4, blocks, chunks, lanes), F32),
        pltpu.VMEM(held, F32),
        pltpu.VMEM(held, F32),
        pltpu.VMEM((2 * nx,) + held, F32),
        pltpu.VMEM((2 * ny,) + held, F32),
        pltpu.VMEM((3,) + held, BF16),
        pltpu.VMEM((nx,) + held, BF16),
        pltpu.VMEM((ny,) + held, BF16),
        pltpu.VMEM((nz,) + held, BF16),
        pltpu.VMEM(held, F32),
        pltpu.VMEM((width // piece, ntp, 2, rows // ntp, piece), BF16),
        pltpu.VMEM((width // piece, ntp - 1, 2, rows // ntp, piece), BF16),
        pltpu.SemaphoreType.DMA((len(args),)),
        pltpu.SemaphoreType.DMA((nx,)),
        pltpu.SemaphoreType.DMA((nx,)),
        pltpu.SemaphoreType.DMA((ny,)),
        pltpu.SemaphoreType.DMA((ny,)),
        pltpu.SemaphoreType.DMA((nz,)),
        pltpu.SemaphoreType.DMA((nz,)),
        pltpu.SemaphoreType.DMA((width // piece, ntp - 1)),
        pltpu.SemaphoreType.DMA((width // piece, ntp - 1)),
    ]
    return pl.pallas_call(
        functools.partial(kernel, ring, ntp, (rows, groups, state, size, width)),
        out_shape=pltpu.VMEM((rows // ntp, width), BF16),
        in_specs=[pl.BlockSpec(memory_space=pl.ANY)] * len(args),
        out_specs=pl.BlockSpec(memory_space=pltpu.VMEM),
        scratch_shapes=scratch,
        compiler_params=pltpu.CompilerParams(
            collective_id=0, has_side_effects=True, vmem_limit_bytes=60 * 1024 * 1024),
        name="mixer",
    )(*args)


def solution(mesh):
    in_specs = (
        P("sp", "tp"),
        P("tp", None),
        P("tp", None),
        P("tp"),
        P("tp", None, None),
        P("tp", None, None),
        P("tp", None, None),
        P("tp", None, None),
        P("tp"),
        P("tp", None),
        P("tp", None),
        P(),
        P(),
    )
    out_specs = P(("sp", "tp"), None)
    body = functools.partial(local, mesh.shape["sp"], mesh.shape["tp"])
    return jax.shard_map(body, mesh=mesh, in_specs=in_specs, out_specs=out_specs, check_vma=False)
```

```python
import functools

import jax
import jax.numpy as jnp
from jax import lax
from jax.experimental import pallas as pl
from jax.experimental.pallas import tpu as pltpu
from jax.sharding import PartitionSpec as P

MESH = pl.DeviceIdType.MESH
F32 = jnp.float32
BF16 = jnp.bfloat16


def iota(shape, dim):
    return lax.broadcasted_iota(jnp.int32, shape, dim)


def cmul(ar, ai, br, bi):
    return ar * br - ai * bi, ar * bi + ai * br


def nt_dot(left, right):
    return lax.dot_general(left, right, (((1,), (1,)), ((), ())), preferred_element_type=F32)


def split_ring(nsp):
    nx = min(4, nsp)
    ny = min(8, nsp // nx)
    return nsp // (nx * ny), ny, nx


def kernel(ring, ntp, dims, *refs):
    nz, ny, nx = ring
    rows, groups, state, size, width = dims
    (x_h, lr_h, li_h, ls_h, br_h, bi_h, cr_h, ci_h, sk_h, vw_h, gw_h, vb_h, gb_h, out_ref,
     x_v, lr_v, li_v, ls_v, br_v, bi_v, cr_v, ci_v, sk_v, vw_v, gw_v, vb_v, gb_v,
     xp_v, zr_v, zi_v, zcat_v, wcat_v, crm_v, cim_v, resp_v, act_v,
     hx_v, fin_v, a_all_v, tab_x, tab_y, msg_v, recv_x, recv_y, recv_z, h_v, part_v, inbox_v,
     in_sem, send_x, got_x, send_y, got_y, send_z, got_z, ready, psend_sem, precv_sem) = refs
    me = lax.axis_index("sp")
    core = lax.axis_index("tp")
    x, y, z = lax.rem(me, nx), lax.rem(me // nx, ny), me // (nx * ny)
    gpb = 128 // size
    lanes = gpb * state
    blocks = groups // gpb
    chunks = 16
    length = rows // chunks
    own_rows = rows // ntp
    tall, wide = fin_v.shape[0] // 2, fin_v.shape[1]
    fold = lanes // wide

    hbm = (ls_h, lr_h, li_h, x_h, br_h, bi_h, cr_h, ci_h, sk_h, vb_h, gb_h, vw_h, gw_h)
    vmem = (ls_v, lr_v, li_v, x_v, br_v, bi_v, cr_v, ci_v, sk_v, vb_v, gb_v, vw_v, gw_v)
    copies = [pltpu.make_async_copy(s, d, in_sem.at[i]) for i, (s, d) in enumerate(zip(hbm, vmem))]
    for c in copies[:6]:
        c.start()

    barrier = pltpu.get_barrier_semaphore()
    for k in range(1, ntp):
        pl.semaphore_signal(barrier, inc=1, device_id=(me, lax.rem(core + k, ntp)), device_id_type=MESH)

    def peer(at, count, stride, k):
        other = lax.rem(at + k, count)
        return other, (me + (other - at) * stride, core)

    lines = ((x, nx, 1), (y, ny, nx), (z, nz, nx * ny))
    for line in lines[:2]:
        for k in range(1, line[1]):
            pl.semaphore_signal(barrier, inc=1, device_id=peer(*line, k)[1], device_id_type=MESH)

    @pl.loop(z + 1, nz)
    def _(d):
        pl.semaphore_signal(barrier, inc=1, device_id=peer(*lines[2], d - z)[1], device_id_type=MESH)

    for c in copies[:3]:
        c.wait()
    eye = iota((groups, groups), 0) == iota((groups, groups), 1)
    step = jnp.exp(jnp.sum(jnp.where(eye, ls_v[...], 0.0), axis=1, keepdims=True))
    lam_r, lam_i = lr_v[...], li_v[...]
    mag = jnp.exp(lam_r * step)
    phase = lam_i * step
    t_r, t_i = mag * jnp.cos(phase), mag * jnp.sin(phase)
    den = lam_r * lam_r + lam_i * lam_i
    n_r = t_r - 1.0
    f_r = (n_r * lam_r + t_i * lam_i) / den
    f_i = (t_i * lam_r - n_r * lam_i) / den

    per = 128 // state
    row8, lane8 = iota((gpb, 128), 0), iota((gpb, 128), 1)

    def flat(value, b):
        sub = value[b * gpb:(b + 1) * gpb]
        dup = jnp.concatenate([sub] * per, axis=1)
        return jnp.concatenate(
            [jnp.sum(jnp.where(row8 == per * j + lane8 // state, dup, 0.0), axis=0, keepdims=True)
             for j in range(gpb // per)], axis=1)

    r0, r1 = iota((rows, rows), 0), iota((rows, rows), 1)
    shuffle = jnp.where(r1 == (r0 % chunks) * length + r0 // chunks, 1.0, 0.0).astype(BF16)
    copies[3].wait()
    xp_v[...] = jnp.dot(shuffle, x_v[...], preferred_element_type=F32).astype(BF16)


    c_mask = iota((128, lanes), 0) // size == iota((128, lanes), 1) // state

    def diagonal(tall):
        return jnp.where(c_mask, jnp.concatenate([tall] * gpb, axis=1), 0.0)

    copies[4].wait()
    copies[5].wait()
    for c in copies[6:]:
        c.start()
    crow = iota((chunks, lanes), 0)

    def shift(value, s):
        return jnp.where(crow >= s, pltpu.roll(value, s, 0), 0.0)

    for b in range(blocks):
        xb = xp_v[:, b * 128:(b + 1) * 128]

        def inject(ref):
            mat = diagonal(ref[b * gpb:(b + 1) * gpb].reshape(128, state)).astype(BF16)
            return jnp.dot(xb, mat, preferred_element_type=F32)

        zr_v[b] = inject(br_v)
        zi_v[b] = inject(bi_v)
        a1r, a1i = flat(t_r, b), flat(t_i, b)
        ar, ai = jnp.broadcast_to(a1r, (chunks, lanes)), jnp.broadcast_to(a1i, (chunks, lanes))
        z_r = z_i = None
        for o in range(length):
            here = pl.ds(o * chunks, chunks)
            if o == 0:
                z_r, z_i = zr_v[b, here, :], zi_v[b, here, :]
            else:
                p_r, p_i = cmul(ar, ai, z_r, z_i)
                z_r, z_i = p_r + zr_v[b, here, :], p_i + zi_v[b, here, :]
                zr_v[b, here, :] = z_r
                zi_v[b, here, :] = z_i
        qr, qi = ar, ai
        s = 1
        while s < length:
            qr, qi = cmul(qr, qi, qr, qi)
            s *= 2
        pw_r, pw_i = jnp.ones_like(qr), jnp.zeros_like(qr)
        s = 1
        while s < chunks:
            m_r, m_i = cmul(qr, qi, shift(z_r, s), shift(z_i, s))
            z_r, z_i = z_r + m_r, z_i + m_i
            bit = (crow // s) % 2 == 1
            pw_r, pw_i = cmul(pw_r, pw_i, jnp.where(bit, qr, 1.0), jnp.where(bit, qi, 0.0))
            qr, qi = cmul(qr, qi, qr, qi)
            s *= 2
        hx_v[0, b], hx_v[1, b] = shift(z_r, 1), shift(z_i, 1)
        for ref, val_r, val_i in ((fin_v, z_r[chunks - 1:], z_i[chunks - 1:]), (a_all_v, qr[:1], qi[:1])):
            for u in range(fold):
                at, cols = b * fold + u, slice(u * wide, (u + 1) * wide)
                ref[at:at + 1] = val_r[:, cols]
                ref[tall + at:tall + at + 1] = val_i[:, cols]
        hx_v[2, b], hx_v[3, b] = pw_r, pw_i
    msg_v[0] = fin_v[...].astype(BF16)

    pl.semaphore_wait(barrier, nx - 1 + ny - 1 + ntp - 1 + z)

    @pl.loop(0, z)
    def _(d):
        pl.semaphore_signal(ready.at[z], inc=1, device_id=peer(*lines[2], d - z + nz)[1], device_id_type=MESH)

    def outgoing(stage, k):
        at = lines[stage][0]
        other, device = peer(*lines[stage], k)
        return pltpu.make_async_remote_copy(
            src_ref=msg_v.at[stage], dst_ref=(recv_x, recv_y, recv_z)[stage].at[at],
            send_sem=(send_x, send_y, send_z)[stage].at[other], recv_sem=(got_x, got_y, got_z)[stage].at[at],
            device_id=device, device_id_type=MESH)

    def incoming(stage, k):
        other, device = peer(*lines[stage], k)
        recv = (recv_x, recv_y, recv_z)[stage].at[other]
        pltpu.make_async_remote_copy(
            src_ref=msg_v.at[stage], dst_ref=recv,
            send_sem=(send_x, send_y, send_z)[stage].at[other], recv_sem=(got_x, got_y, got_z)[stage].at[other],
            device_id=device, device_id_type=MESH).wait_recv()
        got = recv[...].astype(F32)
        return other, got[:tall], got[tall:]

    def near_first(count):
        return sorted(range(1, count), key=lambda k: min(k, count - k))

    for k in reversed(near_first(nx)):
        outgoing(0, k).start()

    def powers(tab, count, a_r, a_i):
        p_r, p_i = jnp.ones((tall, wide), F32), jnp.zeros((tall, wide), F32)
        for i in range(count):
            tab[i] = jnp.zeros((2 * tall, wide), F32)
            tab[count + i, :tall], tab[count + i, tall:] = p_r, p_i
            p_r, p_i = cmul(p_r, p_i, a_r, a_i)
        return p_r, p_i

    ax_r, ax_i = powers(tab_x, nx, a_all_v[:tall], a_all_v[tall:])
    ay_r, ay_i = powers(tab_y, ny, ax_r, ax_i)

    def weight(tab, at, v_r, v_i):
        return cmul(tab[at, :tall], tab[at, tall:], v_r, v_i)

    def collect(stage, tab, own_r, own_i):
        at, count, _ = lines[stage]
        t_r, t_i = weight(tab, count + count - 1 - at, own_r, own_i)
        p_r = p_i = jnp.zeros((tall, wide), F32)
        for k in near_first(count):
            other, v_r, v_i = incoming(stage, k)
            m_r, m_i = weight(tab, count + count - 1 - other, v_r, v_i)
            t_r, t_i = t_r + m_r, t_i + m_i
            m_r, m_i = weight(tab, count + at - 1 - other, v_r, v_i)
            p_r, p_i = p_r + m_r, p_i + m_i
        return t_r, t_i, p_r, p_i

    copies[6].wait()
    copies[7].wait()
    copies[8].wait()
    def respond(b):
        a1r, a1i = flat(t_r, b), flat(t_i, b)
        ar, ai = jnp.broadcast_to(a1r, (chunks, lanes)), jnp.broadcast_to(a1i, (chunks, lanes))
        w_r, w_i = hx_v[0, b], hx_v[1, b]
        p_r, p_i = hx_v[2, b], hx_v[3, b]
        for o in range(length):
            here = pl.ds(o * chunks, chunks)
            w_r, w_i = cmul(ar, ai, w_r, w_i)
            p_r, p_i = cmul(ar, ai, p_r, p_i)
            zcat_v[here, :lanes] = (zr_v[b, here, :] + w_r).astype(BF16)
            zcat_v[here, lanes:] = (zi_v[b, here, :] + w_i).astype(BF16)
            wcat_v[b, here, :lanes] = p_r.astype(BF16)
            wcat_v[b, here, lanes:] = p_i.astype(BF16)
        gains_r, gains_i = [], []
        for g in range(b * gpb, (b + 1) * gpb):
            g_r, g_i = cmul(cr_v[g], ci_v[g], f_r[g:g + 1], f_i[g:g + 1])
            gains_r.append(g_r)
            gains_i.append(g_i)

        m_r = diagonal(jnp.concatenate(gains_r, axis=0))
        m_i = diagonal(jnp.concatenate(gains_i, axis=0))
        crm_v[b], cim_v[b] = m_r, m_i
        mats = jnp.concatenate([m_r.astype(BF16), (-m_i).astype(BF16)], axis=1)
        col = pl.ds(b * 128, 128)
        resp_v[:, col] = nt_dot(zcat_v[...], mats) + sk_v[:, col] * xp_v[:, col].astype(F32)

    half = blocks // 2
    for b in range(half):
        respond(b)
    row_r, row_i, hx_r, hx_i = collect(0, tab_x, fin_v[:tall], fin_v[tall:])
    msg_v[1, :tall], msg_v[1, tall:] = row_r.astype(BF16), row_i.astype(BF16)
    for k in reversed(near_first(ny)):
        outgoing(1, k).start()
    for b in range(half, blocks):
        respond(b)
    plane_r, plane_i, hy_r, hy_i = collect(1, tab_y, row_r, row_i)
    msg_v[2, :tall], msg_v[2, tall:] = plane_r.astype(BF16), plane_i.astype(BF16)

    @pl.loop(z + 1, nz)
    def _(d):
        pl.semaphore_wait(ready.at[d], 1)
        outgoing(2, d - z).start()

    m_r, m_i = weight(tab_x, nx + x, hy_r, hy_i)
    h_r, h_i = hx_r + m_r, hx_i + m_i
    s_r, s_i = weight(tab_x, nx + x, tab_y[ny + y, :tall], tab_y[ny + y, tall:])

    def gather(k, carry):
        h_r, h_i, p_r, p_i = carry
        _, v_r, v_i = incoming(2, nz - 1 - k)
        m_r, m_i = cmul(p_r, p_i, v_r, v_i)
        return (h_r + m_r, h_i + m_i) + cmul(p_r, p_i, ay_r, ay_i)

    h_r, h_i, _, _ = lax.fori_loop(0, z, gather, (h_r, h_i, s_r, s_i))
    h_v[:tall] = h_r
    h_v[tall:] = h_i

    def flat_h(at, b):
        return jnp.concatenate([h_v[at + b * fold + u:at + b * fold + u + 1] for u in range(fold)], axis=1)

    for b in range(blocks):
        k_r, k_i = cmul(crm_v[b], cim_v[b], flat_h(0, b), flat_h(tall, b))
        mats = jnp.concatenate([k_r.astype(BF16), (-k_i).astype(BF16)], axis=1)
        col = pl.ds(b * 128, 128)
        total = resp_v[:, col] + nt_dot(wcat_v[b], mats)
        act_v[:, col] = jax.nn.gelu(total).astype(BF16)

    back = jnp.where(r1 == (r0 % length) * chunks + r0 // length, 1.0, 0.0).astype(BF16)
    act = jnp.dot(back, act_v[...], preferred_element_type=F32).astype(BF16)

    for c in copies[9:]:
        c.wait()
    piece = inbox_v.shape[-1]
    pieces = width // piece

    def exchange(j, k):
        to = lax.rem(core + k, ntp)
        return pltpu.make_async_remote_copy(
            src_ref=part_v.at[j, to], dst_ref=inbox_v.at[j, k - 1],
            send_sem=psend_sem.at[j, k - 1], recv_sem=precv_sem.at[j, k - 1],
            device_id=(me, to), device_id_type=MESH)

    for j in range(pieces):
        col = pl.ds(j * piece, piece)
        for which, weight in enumerate((vw_v, gw_v)):
            part = jnp.dot(act, weight[:, col], preferred_element_type=F32).astype(BF16)
            for i in range(ntp):
                part_v[j, i, which] = part[i * own_rows:(i + 1) * own_rows]
        for k in range(1, ntp):
            exchange(j, k).start()
    for j in range(pieces):
        col = pl.ds(j * piece, piece)
        for k in range(1, ntp):
            exchange(j, k).wait_recv()
        sums = []
        for which, bias in enumerate((vb_v, gb_v)):
            total = part_v[j, core, which].astype(F32)
            for k in range(1, ntp):
                total = total + inbox_v[j, k - 1, which].astype(F32)
            sums.append(total + bias[:, col])
        out_ref[:, col] = (sums[0] * jax.nn.sigmoid(sums[1])).astype(BF16)
    for j in range(pieces):
        for k in range(1, ntp):
            exchange(j, k).wait_send()

    for stage in range(2):
        for k in range(1, lines[stage][1]):
            outgoing(stage, k).wait_send()

    @pl.loop(z + 1, nz)
    def _(d):
        outgoing(2, d - z).wait_send()


def local(nsp, ntp, features, lambda_real, lambda_imag, log_step, input_real, input_imag, real_output,
          imaginary_output, skip_gain, value_weight, gate_weight, value_bias, gate_bias):
    rows, channels = features.shape
    groups, state = lambda_real.shape
    size = input_real.shape[2]
    input_real, input_imag = jnp.swapaxes(input_real, 1, 2), jnp.swapaxes(input_imag, 1, 2)
    width = value_weight.shape[1]
    gpb = 128 // size
    lanes, blocks, chunks = gpb * state, groups // gpb, 16
    piece = min(512, width)
    ring = nz, ny, nx = split_ring(nsp)
    held = (16, 2 * blocks * lanes // 16)
    args = (features, lambda_real, lambda_imag, log_step[None], input_real, input_imag, real_output,
            imaginary_output, skip_gain[None], value_weight, gate_weight, value_bias[None], gate_bias[None])
    scratch = [pltpu.VMEM(a.shape, a.dtype) for a in args]
    scratch += [
        pltpu.VMEM((rows, channels), BF16),
        pltpu.VMEM((blocks, rows, lanes), F32),
        pltpu.VMEM((blocks, rows, lanes), F32),
        pltpu.VMEM((rows, 2 * lanes), BF16),
        pltpu.VMEM((blocks, rows, 2 * lanes), BF16),
        pltpu.VMEM((blocks, 128, lanes), F32),
        pltpu.VMEM((blocks, 128, lanes), F32),
        pltpu.VMEM((rows, channels), F32),
        pltpu.VMEM((rows, channels), BF16),
        pltpu.VMEM((4, blocks, chunks, lanes), F32),
        pltpu.VMEM(held, F32),
        pltpu.VMEM(held, F32),
        pltpu.VMEM((2 * nx,) + held, F32),
        pltpu.VMEM((2 * ny,) + held, F32),
        pltpu.VMEM((3,) + held, BF16),
        pltpu.VMEM((nx,) + held, BF16),
        pltpu.VMEM((ny,) + held, BF16),
        pltpu.VMEM((nz,) + held, BF16),
        pltpu.VMEM(held, F32),
        pltpu.VMEM((width // piece, ntp, 2, rows // ntp, piece), BF16),
        pltpu.VMEM((width // piece, ntp - 1, 2, rows // ntp, piece), BF16),
        pltpu.SemaphoreType.DMA((len(args),)),
        pltpu.SemaphoreType.DMA((nx,)),
        pltpu.SemaphoreType.DMA((nx,)),
        pltpu.SemaphoreType.DMA((ny,)),
        pltpu.SemaphoreType.DMA((ny,)),
        pltpu.SemaphoreType.DMA((nz,)),
        pltpu.SemaphoreType.DMA((nz,)),
        pltpu.SemaphoreType.REGULAR((nz,)),
        pltpu.SemaphoreType.DMA((width // piece, ntp - 1)),
        pltpu.SemaphoreType.DMA((width // piece, ntp - 1)),
    ]
    return pl.pallas_call(
        functools.partial(kernel, ring, ntp, (rows, groups, state, size, width)),
        out_shape=pltpu.VMEM((rows // ntp, width), BF16),
        in_specs=[pl.BlockSpec(memory_space=pl.ANY)] * len(args),
        out_specs=pl.BlockSpec(memory_space=pltpu.VMEM),
        scratch_shapes=scratch,
        compiler_params=pltpu.CompilerParams(
            collective_id=0, has_side_effects=True, vmem_limit_bytes=60 * 1024 * 1024),
        name="mixer",
    )(*args)


def solution(mesh):
    in_specs = (
        P("sp", "tp"),
        P("tp", None),
        P("tp", None),
        P("tp"),
        P("tp", None, None),
        P("tp", None, None),
        P("tp", None, None),
        P("tp", None, None),
        P("tp"),
        P("tp", None),
        P("tp", None),
        P(),
        P(),
    )
    out_specs = P(("sp", "tp"), None)
    body = functools.partial(local, mesh.shape["sp"], mesh.shape["tp"])
    return jax.shard_map(body, mesh=mesh, in_specs=in_specs, out_specs=out_specs, check_vma=False)
```

```python
import functools

import jax
import jax.numpy as jnp
from jax import lax
from jax.experimental import pallas as pl
from jax.experimental.pallas import tpu as pltpu
from jax.sharding import PartitionSpec as P

MESH = pl.DeviceIdType.MESH
F32 = jnp.float32
BF16 = jnp.bfloat16


def iota(shape, dim):
    return lax.broadcasted_iota(jnp.int32, shape, dim)


def cmul(ar, ai, br, bi):
    return ar * br - ai * bi, ar * bi + ai * br


def nt_dot(left, right):
    return lax.dot_general(left, right, (((1,), (1,)), ((), ())), preferred_element_type=F32)


def split_ring(nsp):
    nx = min(4, nsp)
    ny = min(8, nsp // nx)
    return nsp // (nx * ny), ny, nx


def near_first(count):
    return sorted(range(1, count), key=lambda k: min(k, count - k))


def kernel(ring, ntp, dims, *refs):
    nz, ny, nx = ring
    rows, groups, state, size, width = dims
    (x_h, lr_h, li_h, ls_h, br_h, bi_h, cr_h, ci_h, sk_h, vw_h, gw_h, vb_h, gb_h, out_ref,
     x_v, lr_v, li_v, ls_v, br_v, bi_v, cr_v, ci_v, sk_v, vb_v, gb_v, w_v,
     xp_v, bmat_v, mats_v, zr_v, zi_v, zcat_v, wcat_v, gain_v, resp_v, corr_v, act_v, part_v,
     par_v, fin_v, tab_x, tab_y, msg_v, recv_x, recv_y, recv_z, h_v,
     in_sem, w_sem, send_x, got_x, send_y, got_y, send_z, got_z, ready, w_send, w_got, a_send, a_got) = refs
    me = lax.axis_index("sp")
    core = lax.axis_index("tp")
    other_core = 1 - core
    x, y, z = lax.rem(me, nx), lax.rem(me // nx, ny), me // (nx * ny)
    gpb = 128 // size
    lanes = gpb * state
    blocks = groups // gpb
    chunks = 16
    length = rows // chunks
    half = rows // ntp
    tall, wide = fin_v.shape[0] // 2, fin_v.shape[1]
    fold = lanes // wide
    per = 128 // state

    hbm = (x_h, ls_h, lr_h, li_h, br_h, bi_h, cr_h, ci_h, sk_h, vb_h, gb_h)
    vmem = (x_v, ls_v, lr_v, li_v, br_v, bi_v, cr_v, ci_v, sk_v, vb_v, gb_v)
    copies = [pltpu.make_async_copy(s, d, in_sem.at[i]) for i, (s, d) in enumerate(zip(hbm, vmem))]
    for c in copies:
        c.start()
    weights = (vw_h, gw_h)
    own_w = [pltpu.make_async_copy(s, w_v.at[i, core], w_sem.at[i]) for i, s in enumerate(weights)]
    peer_w = [pltpu.make_async_remote_copy(
        src_ref=s, dst_ref=w_v.at[i, core], send_sem=w_send.at[i], recv_sem=w_got.at[i],
        device_id=(me, other_core), device_id_type=MESH) for i, s in enumerate(weights)]
    got_w = [pltpu.make_async_remote_copy(
        src_ref=s, dst_ref=w_v.at[i, other_core], send_sem=w_send.at[i], recv_sem=w_got.at[i],
        device_id=(me, other_core), device_id_type=MESH) for i, s in enumerate(weights)]

    barrier = pltpu.get_barrier_semaphore()
    pl.semaphore_signal(barrier, inc=1, device_id=(me, other_core), device_id_type=MESH)

    def peer(at, count, stride, k):
        other = lax.rem(at + k, count)
        return other, (me + (other - at) * stride, core)

    lines = ((x, nx, 1), (y, ny, nx), (z, nz, nx * ny))
    for line in lines[:2]:
        for k in range(1, line[1]):
            pl.semaphore_signal(barrier, inc=1, device_id=peer(*line, k)[1], device_id_type=MESH)

    @pl.loop(z + 1, nz)
    def _(d):
        pl.semaphore_signal(barrier, inc=1, device_id=peer(*lines[2], d - z)[1], device_id_type=MESH)

    bmat_v[...] = jnp.zeros_like(bmat_v)
    pair_mask = [iota((size, 128), 1) // state == i for i in range(per)]

    def spread(value, g):
        return jnp.where(pair_mask[g % per], jnp.concatenate([value] * per, axis=1), 0.0)

    for c in copies[1:4]:
        c.wait()
    eye = iota((groups, groups), 0) == iota((groups, groups), 1)
    step = jnp.exp(jnp.sum(jnp.where(eye, ls_v[...], 0.0), axis=1, keepdims=True))
    lam_r, lam_i = lr_v[...], li_v[...]
    mag = jnp.exp(lam_r * step)
    phase = lam_i * step
    t_r, t_i = mag * jnp.cos(phase), mag * jnp.sin(phase)
    den = lam_r * lam_r + lam_i * lam_i
    n_r = t_r - 1.0
    f_r = (n_r * lam_r + t_i * lam_i) / den
    f_i = (t_i * lam_r - n_r * lam_i) / den

    row8, lane8 = iota((gpb, 128), 0), iota((gpb, 128), 1)

    def hold(at, value):
        for b in range(blocks):
            dup = jnp.concatenate([value[b * gpb:(b + 1) * gpb]] * per, axis=1)
            for j in range(gpb // per):
                tile = jnp.sum(jnp.where(row8 == per * j + lane8 // state, dup, 0.0), axis=0, keepdims=True)
                flat = j * 128
                r, c = b * fold + flat // wide, flat % wide
                par_v[at, r:r + 1, c:c + 128] = tile

    hold(0, t_r)
    hold(1, t_i)
    hold(2, f_r)
    hold(3, f_i)

    def pair(k):
        return par_v[2 * k], par_v[2 * k + 1]

    q_r, q_i = pair(0)
    squares = rows.bit_length() - 1
    for k in range(squares):
        q_r, q_i = cmul(q_r, q_i, q_r, q_i)
        par_v[4 + 2 * k] = q_r
        par_v[5 + 2 * k] = q_i

    def row(k, b):
        return [jnp.concatenate([par_v[2 * k + i, b * fold + u:b * fold + u + 1] for u in range(fold)], axis=1)
                for i in range(2)]

    def power(exponent, b):
        return row(0 if exponent == 1 else exponent.bit_length(), b)

    row_b = iota((8, lanes), 0)

    def eight(b, flip):
        count = 7 - row_b if flip else row_b
        v_r, v_i = jnp.ones((8, lanes), F32), jnp.zeros((8, lanes), F32)
        for k in range(3):
            bit = (count // (1 << k)) % 2 == 1
            s_r, s_i = power(1 << k, b)
            v_r, v_i = cmul(v_r, v_i, jnp.where(bit, s_r, 1.0), jnp.where(bit, s_i, 0.0))
        return v_r, v_i

    copies[4].wait()
    copies[5].wait()
    for g in range(groups):
        b, l = g // gpb, g % gpb
        at, cols = slice(l * size, (l + 1) * size), l // per * 128
        bmat_v[b, at, cols:cols + 128] = spread(br_v[g], g).astype(BF16)
        bmat_v[b, at, lanes + cols:lanes + cols + 128] = spread(bi_v[g], g).astype(BF16)
    copies[0].wait()

    def inject(source, b):
        out = jnp.dot(source[:, b * 128:(b + 1) * 128], bmat_v[b], preferred_element_type=F32)
        zr_v[b] = out[:, :lanes]
        zi_v[b] = out[:, lanes:]

    for b in range(blocks):
        inject(x_v, b)
    for b in range(blocks):
        e_r, e_i = power(8, b)
        ends = []
        steps = rows // 16
        for h in range(2):
            z_r, z_i = zr_v[b, h * half:h * half + 8, :], zi_v[b, h * half:h * half + 8, :]
            for k in range(1, steps):
                here = pl.ds(h * half + 8 * k, 8)
                p_r, p_i = cmul(e_r, e_i, z_r, z_i)
                z_r, z_i = p_r + zr_v[b, here, :], p_i + zi_v[b, here, :]
            ends.append((z_r, z_i))
        p_r, p_i = cmul(*power(rows // 2, b), *ends[0])
        v_r, v_i = cmul(*eight(b, True), p_r + ends[1][0], p_i + ends[1][1])
        v_r, v_i = jnp.sum(v_r, axis=0, keepdims=True), jnp.sum(v_i, axis=0, keepdims=True)
        for u in range(fold):
            at, cols = b * fold + u, slice(u * wide, (u + 1) * wide)
            fin_v[at:at + 1] = v_r[:, cols]
            fin_v[tall + at:tall + at + 1] = v_i[:, cols]
    msg_v[0] = fin_v[...].astype(BF16)

    pl.semaphore_wait(barrier, nx - 1 + ny - 1 + ntp - 1 + z)

    def outgoing(stage, k):
        at = lines[stage][0]
        other, device = peer(*lines[stage], k)
        return pltpu.make_async_remote_copy(
            src_ref=msg_v.at[stage], dst_ref=(recv_x, recv_y, recv_z)[stage].at[at],
            send_sem=(send_x, send_y, send_z)[stage].at[other], recv_sem=(got_x, got_y, got_z)[stage].at[at],
            device_id=device, device_id_type=MESH)

    def incoming(stage, k):
        other, device = peer(*lines[stage], k)
        recv = (recv_x, recv_y, recv_z)[stage].at[other]
        pltpu.make_async_remote_copy(
            src_ref=msg_v.at[stage], dst_ref=recv,
            send_sem=(send_x, send_y, send_z)[stage].at[other], recv_sem=(got_x, got_y, got_z)[stage].at[other],
            device_id=device, device_id_type=MESH).wait_recv()
        got = recv[...].astype(F32)
        return other, got[:tall], got[tall:]

    for k in reversed(near_first(nx)):
        outgoing(0, k).start()

    @pl.loop(0, z)
    def _(d):
        pl.semaphore_signal(ready.at[z], inc=1, device_id=peer(*lines[2], d - z + nz)[1], device_id_type=MESH)

    for c in own_w + peer_w:
        c.start()

    def powers(tab, count, a_r, a_i):
        p_r, p_i = jnp.ones((tall, wide), F32), jnp.zeros((tall, wide), F32)
        for i in range(count):
            tab[i] = jnp.zeros((2 * tall, wide), F32)
            tab[count + i, :tall], tab[count + i, tall:] = p_r, p_i
            p_r, p_i = cmul(p_r, p_i, a_r, a_i)
        return p_r, p_i

    ax_r, ax_i = powers(tab_x, nx, q_r, q_i)
    ay_r, ay_i = powers(tab_y, ny, ax_r, ax_i)

    def weight(tab, at, v_r, v_i):
        return cmul(tab[at, :tall], tab[at, tall:], v_r, v_i)

    def collect(stage, tab, own_r, own_i):
        at, count, _ = lines[stage]
        t_r, t_i = weight(tab, count + count - 1 - at, own_r, own_i)
        p_r = p_i = jnp.zeros((tall, wide), F32)
        for k in near_first(count):
            other, v_r, v_i = incoming(stage, k)
            m_r, m_i = weight(tab, count + count - 1 - other, v_r, v_i)
            t_r, t_i = t_r + m_r, t_i + m_i
            m_r, m_i = weight(tab, count + at - 1 - other, v_r, v_i)
            p_r, p_i = p_r + m_r, p_i + m_i
        return t_r, t_i, p_r, p_i

    mats_v[...] = jnp.zeros_like(mats_v)
    r0, r1 = iota((rows, rows), 0), iota((rows, rows), 1)
    shuffle = jnp.where(r1 == (r0 % chunks) * length + r0 // chunks, 1.0, 0.0).astype(BF16)
    back = jnp.where(r1 == (r0 % length) * chunks + r0 // length, 1.0, 0.0).astype(BF16)
    xp_v[...] = jnp.dot(shuffle, x_v[...], preferred_element_type=F32).astype(BF16)
    crow = iota((chunks, lanes), 0)

    def shift(value, s):
        return jnp.where(crow >= s, pltpu.roll(value, s, 0), 0.0)

    copies[6].wait()
    copies[7].wait()
    copies[8].wait()

    def place(b, slot, l, v_r, v_i):
        at, cols = slot * 128 + l * size, l // per * 128
        mats_v[b, at:at + size, cols:cols + 128] = v_r.astype(BF16)
        mats_v[b, at:at + size, lanes + cols:lanes + cols + 128] = (-v_i).astype(BF16)

    def respond(b):
        inject(xp_v, b)
        a_r, a_i = power(1, b)
        z_r, z_i = zr_v[b, :chunks, :], zi_v[b, :chunks, :]
        for o in range(1, length):
            here = pl.ds(o * chunks, chunks)
            p_r, p_i = cmul(a_r, a_i, z_r, z_i)
            z_r, z_i = p_r + zr_v[b, here, :], p_i + zi_v[b, here, :]
            zr_v[b, here, :] = z_r
            zi_v[b, here, :] = z_i
        s = 1
        while s < chunks:
            m_r, m_i = cmul(*power(length * s, b), shift(z_r, s), shift(z_i, s))
            z_r, z_i = z_r + m_r, z_i + m_i
            s *= 2
        w_r, w_i = shift(z_r, 1), shift(z_i, 1)
        for o in range(length):
            here = pl.ds(o * chunks, chunks)
            w_r, w_i = cmul(a_r, a_i, w_r, w_i)
            zcat_v[b, here, :lanes] = (zr_v[b, here, :] + w_r).astype(BF16)
            zcat_v[b, here, lanes:] = (zi_v[b, here, :] + w_i).astype(BF16)
        e_r, e_i = power(8, b)
        v_r, v_i = cmul(a_r, a_i, *eight(b, False))
        for o in range(half // 16):
            n_r, n_i = cmul(e_r, e_i, v_r, v_i)
            here = pl.ds(o * 16, 16)
            wcat_v[b, here, :lanes] = jnp.concatenate([v_r, n_r], axis=0).astype(BF16)
            wcat_v[b, here, lanes:] = jnp.concatenate([v_i, n_i], axis=0).astype(BF16)
            v_r, v_i = cmul(e_r, e_i, n_r, n_i)
        g_r, g_i = row(1, b)
        for l in range(gpb):
            g, cols = b * gpb + l, slice(l // per * 128, l // per * 128 + 128)
            c_r, c_i = cmul(spread(cr_v[g], g), spread(ci_v[g], g), g_r[:, cols], g_i[:, cols])
            gain_v[0, g], gain_v[1, g] = c_r, c_i
            place(b, 0, l, c_r, c_i)
        col = pl.ds(b * 128, 128)
        out = nt_dot(zcat_v[b], mats_v[b, :128])
        high = out.astype(BF16)
        low = (out - high.astype(F32)).astype(BF16)
        turned = jnp.dot(back, jnp.concatenate([high, low], axis=1), preferred_element_type=F32)
        resp_v[:, col] = turned[:, :128] + turned[:, 128:] + sk_v[:, col] * x_v[:, col].astype(F32)

    for b in range(blocks // 2):
        respond(b)
    row_r, row_i, hx_r, hx_i = collect(0, tab_x, fin_v[:tall], fin_v[tall:])
    msg_v[1, :tall], msg_v[1, tall:] = row_r.astype(BF16), row_i.astype(BF16)
    for k in reversed(near_first(ny)):
        outgoing(1, k).start()
    for b in range(blocks // 2, blocks):
        respond(b)
    plane_r, plane_i, hy_r, hy_i = collect(1, tab_y, row_r, row_i)
    msg_v[2, :tall], msg_v[2, tall:] = plane_r.astype(BF16), plane_i.astype(BF16)

    @pl.loop(z + 1, nz)
    def _(d):
        pl.semaphore_wait(ready.at[d], 1)
        outgoing(2, d - z).start()

    m_r, m_i = weight(tab_x, nx + x, hy_r, hy_i)
    h_r, h_i = hx_r + m_r, hx_i + m_i
    s_r, s_i = weight(tab_x, nx + x, tab_y[ny + y, :tall], tab_y[ny + y, tall:])

    def gather(k, carry):
        h_r, h_i, p_r, p_i = carry
        _, v_r, v_i = incoming(2, nz - 1 - k)
        m_r, m_i = cmul(p_r, p_i, v_r, v_i)
        return (h_r + m_r, h_i + m_i) + cmul(p_r, p_i, ay_r, ay_i)

    h_r, h_i, _, _ = lax.fori_loop(0, z, gather, (h_r, h_i, s_r, s_i))
    late_r, late_i = cmul(*pair(1 + (half.bit_length() - 1)), h_r, h_i)
    for slot, is_late in enumerate((core == 0, core == 1)):
        h_v[slot, :tall] = jnp.where(is_late, late_r, h_r)
        h_v[slot, tall:] = jnp.where(is_late, late_i, h_i)

    def start_of(who):
        return pl.multiple_of(who * half, half)

    for b in range(blocks):
        for slot in range(ntp):
            for l in range(gpb):
                g, flat = b * gpb + l, l // per * 128
                r, cols = b * fold + flat // wide, slice(flat % wide, flat % wide + 128)
                place(b, 1 + slot, l, *cmul(
                    gain_v[0, g], gain_v[1, g], h_v[slot, r:r + 1, cols], h_v[slot, tall + r:tall + r + 1, cols]))
        col = pl.ds(b * 128, 128)
        corr = nt_dot(wcat_v[b], mats_v[b, 128:])
        corr_v[:, col] = corr[:, 128:]
        act_v[0, :, col] = jax.nn.gelu(corr[:, :128] + resp_v[pl.ds(start_of(other_core), half), col]).astype(BF16)
    exchange = pltpu.make_async_remote_copy(
        src_ref=act_v.at[0], dst_ref=act_v.at[2], send_sem=a_send, recv_sem=a_got,
        device_id=(me, other_core), device_id_type=MESH)
    exchange.start()
    act_v[1] = jax.nn.gelu(corr_v[...] + resp_v[pl.ds(start_of(core), half), :]).astype(BF16)
    copies[9].wait()
    copies[10].wait()
    for c in own_w:
        c.wait()
    piece = min(512, width)
    cols_of = [pl.ds(j * piece, piece) for j in range(width // piece)]
    for col in cols_of:
        for i in range(2):
            part_v[i, :, col] = jnp.dot(act_v[1], w_v[i, core, :, col], preferred_element_type=F32)
    for c in got_w:
        c.wait_recv()
    exchange.wait_recv()
    for col in cols_of:
        sums = [part_v[i, :, col] + bias[:, col]
                + jnp.dot(act_v[2], w_v[i, other_core, :, col], preferred_element_type=F32)
                for i, bias in enumerate((vb_v, gb_v))]
        out_ref[:, col] = (sums[0] * jax.nn.sigmoid(sums[1])).astype(BF16)
    exchange.wait_send()
    for c in peer_w:
        c.wait_send()
    for stage in range(2):
        for k in range(1, lines[stage][1]):
            outgoing(stage, k).wait_send()

    @pl.loop(z + 1, nz)
    def _(d):
        outgoing(2, d - z).wait_send()


def local(nsp, ntp, features, lambda_real, lambda_imag, log_step, input_real, input_imag, real_output,
          imaginary_output, skip_gain, value_weight, gate_weight, value_bias, gate_bias):
    rows, channels = features.shape
    groups, state = lambda_real.shape
    size = input_real.shape[2]
    input_real, input_imag = jnp.swapaxes(input_real, 1, 2), jnp.swapaxes(input_imag, 1, 2)
    width = value_weight.shape[1]
    gpb = 128 // size
    lanes, blocks = gpb * state, groups // gpb
    ring = nz, ny, nx = split_ring(nsp)
    held = (16, 2 * blocks * lanes // 16)
    single = (8, held[1])
    half = rows // ntp
    args = (features, lambda_real, lambda_imag, log_step[None], input_real, input_imag, real_output,
            imaginary_output, skip_gain[None], value_weight, gate_weight, value_bias[None], gate_bias[None])
    scratch = [pltpu.VMEM(a.shape, a.dtype) for a in args[:9] + args[11:]]
    scratch += [
        pltpu.VMEM((2, ntp, channels, width), BF16),
        pltpu.VMEM((rows, channels), BF16),
        pltpu.VMEM((blocks, 128, 2 * lanes), BF16),
        pltpu.VMEM((blocks, 3 * 128, 2 * lanes), BF16),
        pltpu.VMEM((blocks, rows, lanes), F32),
        pltpu.VMEM((blocks, rows, lanes), F32),
        pltpu.VMEM((blocks, rows, 2 * lanes), BF16),
        pltpu.VMEM((blocks, half, 2 * lanes), BF16),
        pltpu.VMEM((2, groups, size, 128), F32),
        pltpu.VMEM((rows, channels), F32),
        pltpu.VMEM((half, channels), F32),
        pltpu.VMEM((3, half, channels), BF16),
        pltpu.VMEM((2, half, width), F32),
        pltpu.VMEM((4 + 2 * (rows.bit_length() - 1),) + single, F32),
        pltpu.VMEM(held, F32),
        pltpu.VMEM((2 * nx,) + held, F32),
        pltpu.VMEM((2 * ny,) + held, F32),
        pltpu.VMEM((3,) + held, BF16),
        pltpu.VMEM((nx,) + held, BF16),
        pltpu.VMEM((ny,) + held, BF16),
        pltpu.VMEM((nz,) + held, BF16),
        pltpu.VMEM((ntp,) + held, F32),
        pltpu.SemaphoreType.DMA((11,)),
        pltpu.SemaphoreType.DMA((2,)),
        pltpu.SemaphoreType.DMA((nx,)),
        pltpu.SemaphoreType.DMA((nx,)),
        pltpu.SemaphoreType.DMA((ny,)),
        pltpu.SemaphoreType.DMA((ny,)),
        pltpu.SemaphoreType.DMA((nz,)),
        pltpu.SemaphoreType.DMA((nz,)),
        pltpu.SemaphoreType.REGULAR((nz,)),
        pltpu.SemaphoreType.DMA((2,)),
        pltpu.SemaphoreType.DMA((2,)),
        pltpu.SemaphoreType.DMA,
        pltpu.SemaphoreType.DMA,
    ]
    return pl.pallas_call(
        functools.partial(kernel, ring, ntp, (rows, groups, state, size, width)),
        out_shape=pltpu.VMEM((rows // ntp, width), BF16),
        in_specs=[pl.BlockSpec(memory_space=pl.ANY)] * len(args),
        out_specs=pl.BlockSpec(memory_space=pltpu.VMEM),
        scratch_shapes=scratch,
        compiler_params=pltpu.CompilerParams(
            collective_id=0, has_side_effects=True, vmem_limit_bytes=60 * 1024 * 1024),
        name="mixer",
    )(*args)


def solution(mesh):
    in_specs = (
        P("sp", "tp"),
        P("tp", None),
        P("tp", None),
        P("tp"),
        P("tp", None, None),
        P("tp", None, None),
        P("tp", None, None),
        P("tp", None, None),
        P("tp"),
        P("tp", None),
        P("tp", None),
        P(),
        P(),
    )
    out_specs = P(("sp", "tp"), None)
    body = functools.partial(local, mesh.shape["sp"], mesh.shape["tp"])
    return jax.shard_map(body, mesh=mesh, in_specs=in_specs, out_specs=out_specs, check_vma=False)
```

```python
import functools

import jax
import jax.numpy as jnp
from jax import lax
from jax.experimental import pallas as pl
from jax.experimental.pallas import tpu as pltpu
from jax.sharding import PartitionSpec as P

MESH = pl.DeviceIdType.MESH
F32 = jnp.float32
BF16 = jnp.bfloat16


def iota(shape, dim):
    return lax.broadcasted_iota(jnp.int32, shape, dim)


def cmul(ar, ai, br, bi):
    return ar * br - ai * bi, ar * bi + ai * br


def nt_dot(left, right):
    return lax.dot_general(left, right, (((1,), (1,)), ((), ())), preferred_element_type=F32)


def split_ring(nsp):
    nx = min(4, nsp)
    ny = min(8, nsp // nx)
    return nsp // (nx * ny), ny, nx


def near_first(count):
    return sorted(range(1, count), key=lambda k: min(k, count - k))


def kernel(ring, ntp, dims, *refs):
    nz, ny, nx = ring
    rows, groups, state, size, width = dims
    (x_h, lr_h, li_h, ls_h, br_h, bi_h, cr_h, ci_h, sk_h, vw_h, gw_h, vb_h, gb_h, out_ref,
     x_v, lr_v, li_v, ls_v, br_v, bi_v, cr_v, ci_v, sk_v, vb_v, gb_v, w_v,
     xp_v, bmat_v, mats_v, keep_v, zr_v, zi_v, zcat_v, wcat_v, gain_v, resp_v, both_v, act_v,
     par_v, fin_v, tab_x, tab_y, sum_v, end_v, row_v, plane_v, recv_x, recv_y, recv_z, h_v, pass_v,
     in_sem, w_sem, send_x, got_x, send_y, got_y, send_z, got_z, ready, d_send, d_got) = refs
    me = lax.axis_index("sp")
    core = lax.axis_index("tp")
    other_core = 1 - core
    x, y, z = lax.rem(me, nx), lax.rem(me // nx, ny), me // (nx * ny)
    gpb = 128 // size
    lanes = gpb * state
    blocks = groups // gpb
    chunks = 16
    length = rows // chunks
    half = rows // ntp
    tall, wide = fin_v.shape[0] // 2, fin_v.shape[1]
    span = ntp * tall
    lead = ntp - 1
    fold = lanes // wide
    per = 128 // state

    quarter = rows // 4
    moves = [(ls_h, ls_v), (lr_h, lr_v), (li_h, li_v)]
    moves += [(x_h.at[pl.ds(i * quarter, quarter)], x_v.at[pl.ds(i * quarter, quarter)]) for i in range(4)]
    moves += [(s.at[pl.ds(i * groups // 2, groups // 2)], d.at[pl.ds(i * groups // 2, groups // 2)])
              for s, d in ((br_h, br_v), (bi_h, bi_v)) for i in range(2)]
    moves += [(cr_h, cr_v), (ci_h, ci_v), (sk_h, sk_v), (vb_h, vb_v), (gb_h, gb_v)]
    copies = [pltpu.make_async_copy(s, d, in_sem.at[i]) for i, (s, d) in enumerate(moves)]
    for c in copies:
        c.start()
    depth = vw_h.shape[0]

    def place_of(who):
        return pl.ds(pl.multiple_of(who * depth, depth), depth)

    def rows_of(who):
        return pl.ds(pl.multiple_of(who * half, half), half)

    weights = (vw_h, gw_h)
    own_w = [pltpu.make_async_copy(s, w_v.at[i, place_of(core)], w_sem.at[i]) for i, s in enumerate(weights)]

    def across(i, src, dst):
        return pltpu.make_async_remote_copy(
            src_ref=src, dst_ref=dst, send_sem=d_send.at[i], recv_sem=d_got.at[i],
            device_id=(me, other_core), device_id_type=MESH)

    out_w = [across(i, s, w_v.at[i, place_of(core)]) for i, s in enumerate(weights)]
    got_w = [across(i, s, w_v.at[i, place_of(other_core)]) for i, s in enumerate(weights)]
    out_par, got_par = (across(2, par_v.at[i], par_v.at[i]) for i in (core, other_core))
    out_gain, got_gain = (across(3, gain_v.at[i], gain_v.at[i]) for i in (core, other_core))
    out_resp = across(4, resp_v.at[rows_of(other_core)], both_v.at[core])
    got_resp = across(4, resp_v.at[rows_of(other_core)], both_v.at[other_core])
    out_h = across(5, pass_v, h_v)

    barrier = pltpu.get_barrier_semaphore()

    def hello(device):
        pl.semaphore_signal(barrier, inc=1, device_id=device, device_id_type=MESH)

    def peer(at, count, stride, k):
        other = lax.rem(at + k, count)
        return other, me + (other - at) * stride

    hello((me, other_core))
    lines = ((x, nx, 1), (y, ny, nx), (z, nz, nx * ny))

    @pl.when(core == lead)
    def _():
        for k in range(1, nx):
            for i in range(ntp):
                hello((peer(*lines[0], k)[1], i))
        for k in range(1, ny):
            hello((peer(*lines[1], k)[1], lead))

        @pl.loop(z + 1, nz)
        def _(d):
            hello((peer(*lines[2], d - z)[1], lead))

    bmat_v[...] = jnp.zeros_like(bmat_v)
    pair_mask = [iota((size, 128), 1) // state == i for i in range(per)]

    def spread(value, g):
        return jnp.where(pair_mask[g % per], jnp.concatenate([value] * per, axis=1), 0.0)

    for c in copies[:3]:
        c.wait()
    eye = iota((groups, groups), 0) == iota((groups, groups), 1)
    step = jnp.exp(jnp.sum(jnp.where(eye, ls_v[...], 0.0), axis=1, keepdims=True))
    lam_r, lam_i = lr_v[...], li_v[...]
    mag = jnp.exp(lam_r * step)
    phase = lam_i * step
    t_r, t_i = mag * jnp.cos(phase), mag * jnp.sin(phase)
    den = lam_r * lam_r + lam_i * lam_i
    n_r = t_r - 1.0
    f_r = (n_r * lam_r + t_i * lam_i) / den
    f_i = (t_i * lam_r - n_r * lam_i) / den

    row8, lane8 = iota((gpb, 128), 0), iota((gpb, 128), 1)

    def hold(at, value):
        for b in range(blocks):
            dup = jnp.concatenate([value[b * gpb:(b + 1) * gpb]] * per, axis=1)
            for j in range(gpb // per):
                tile = jnp.sum(jnp.where(row8 == per * j + lane8 // state, dup, 0.0), axis=0, keepdims=True)
                flat = j * 128
                r, c = b * fold + flat // wide, flat % wide
                par_v[core, at, r:r + 1, c:c + 128] = tile

    hold(0, t_r)
    hold(1, t_i)
    hold(2, f_r)
    hold(3, f_i)

    q_r, q_i = par_v[core, 0], par_v[core, 1]
    squares = rows.bit_length() - 1
    for k in range(squares):
        q_r, q_i = cmul(q_r, q_i, q_r, q_i)
        par_v[core, 4 + 2 * k] = q_r
        par_v[core, 5 + 2 * k] = q_i

    def row(k, b, who=core):
        return [jnp.concatenate(
            [par_v[who, 2 * k + i, b * fold + u:b * fold + u + 1] for u in range(fold)], axis=1) for i in range(2)]

    def power(exponent, b, who=core):
        return row(0 if exponent == 1 else exponent.bit_length(), b, who)

    def pair(k):
        return [jnp.concatenate([par_v[i, 2 * k + j] for i in range(ntp)], axis=0) for j in range(2)]

    row_b = iota((8, lanes), 0)

    def eight(b, flip, who=core):
        count = 7 - row_b if flip else row_b
        v_r, v_i = jnp.ones((8, lanes), F32), jnp.zeros((8, lanes), F32)
        for k in range(3):
            bit = (count // (1 << k)) % 2 == 1
            s_r, s_i = power(1 << k, b, who)
            v_r, v_i = cmul(v_r, v_i, jnp.where(bit, s_r, 1.0), jnp.where(bit, s_i, 0.0))
        return v_r, v_i

    for c in copies[3:11]:
        c.wait()
    late = 1 + (half.bit_length() - 1)
    for g in range(groups):
        b, l = g // gpb, g % gpb
        at, cols = l * size, l // per * 128
        lane = slice(cols, cols + 128)
        b_r, b_i = spread(br_v[g], g), spread(bi_v[g], g)
        e_r, e_i = row(late, b)
        m_r, m_i = cmul(b_r, b_i, e_r[:, lane], e_i[:, lane])
        for base, v_r, v_i in ((0, m_r, m_i), (128, b_r, b_i)):
            bmat_v[b, base + at:base + at + size, cols:cols + 128] = v_r.astype(BF16)
            bmat_v[b, base + at:base + at + size, lanes + cols:lanes + cols + 128] = v_i.astype(BF16)

    for b in range(blocks):
        cols = slice(b * 128, (b + 1) * 128)
        both = jnp.concatenate([x_v[:half, cols], x_v[half:, cols]], axis=1)
        out = jnp.dot(both, bmat_v[b], preferred_element_type=F32)
        e_r, e_i = power(8, b)
        z_r, z_i = out[:8, :lanes], out[:8, lanes:]
        for k in range(1, half // 8):
            p_r, p_i = cmul(e_r, e_i, z_r, z_i)
            z_r, z_i = p_r + out[8 * k:8 * k + 8, :lanes], p_i + out[8 * k:8 * k + 8, lanes:]
        v_r, v_i = cmul(*eight(b, True), z_r, z_i)
        v_r, v_i = jnp.sum(v_r, axis=0, keepdims=True), jnp.sum(v_i, axis=0, keepdims=True)
        for u in range(fold):
            at, cols = b * fold + u, slice(u * wide, (u + 1) * wide)
            fin_v[at:at + 1] = v_r[:, cols]
            fin_v[tall + at:tall + at + 1] = v_i[:, cols]
    end_v[...] = fin_v[...].astype(BF16)

    def to_row(k):
        other, device = peer(*lines[0], k)
        return pltpu.make_async_remote_copy(
            src_ref=end_v, dst_ref=recv_x.at[x, core], send_sem=send_x.at[other], recv_sem=got_x.at[x, core],
            device_id=(device, lead), device_id_type=MESH)

    def along(stage, k):
        at = lines[stage][0]
        other, device = peer(*lines[stage], k)
        message, recv, sent, got = ((), (row_v, recv_y, send_y, got_y), (plane_v, recv_z, send_z, got_z))[stage]
        return pltpu.make_async_remote_copy(
            src_ref=message, dst_ref=recv.at[at], send_sem=sent.at[other], recv_sem=got.at[at],
            device_id=(device, lead), device_id_type=MESH)

    def arrived(recv, got, sent, at, device):
        pltpu.make_async_remote_copy(
            src_ref=recv.at[at], dst_ref=recv.at[at], send_sem=sent, recv_sem=got.at[at],
            device_id=device, device_id_type=MESH).wait_recv()

    def from_row(k):
        other, device = peer(*lines[0], k)
        parts = []
        for i in range(ntp):
            if k == 0 and i == lead:
                parts.append(fin_v[...])
                continue
            arrived(recv_x, got_x, send_x.at[other], (other, i), (device, i))
            parts.append(recv_x[other, i].astype(F32))
        return (other, jnp.concatenate([p[:tall] for p in parts], axis=0),
                jnp.concatenate([p[tall:] for p in parts], axis=0))

    def from_line(stage, k):
        other, device = peer(*lines[stage], k)
        recv, sent, got = ((), (recv_y, send_y, got_y), (recv_z, send_z, got_z))[stage]
        arrived(recv, got, sent.at[other], other, (device, lead))
        value = recv[other].astype(F32)
        return other, value[:span], value[span:]

    @pl.when(core == lead)
    def _():
        pl.semaphore_wait(barrier, nx - 1 + ny - 1 + ntp - 1 + z)
        for k in reversed(near_first(nx)):
            to_row(k).start()

        @pl.loop(0, z)
        def _(d):
            pl.semaphore_signal(
                ready.at[z], inc=1, device_id=(peer(*lines[2], d - z + nz)[1], lead), device_id_type=MESH)

    @pl.when(core != lead)
    def _():
        pl.semaphore_wait(barrier, nx - 1 + ntp - 1)
        for k in list(reversed(near_first(nx))) + [0]:
            to_row(k).start()

    out_par.start()
    for c in own_w:
        c.start()

    mats_v[...] = jnp.zeros_like(mats_v)
    keep_v[...] = jnp.zeros_like(keep_v)
    for c in copies[11:14]:
        c.wait()

    def place(ref, b, l, v_r, v_i):
        at, cols = l * size, l // per * 128
        ref[b, at:at + size, cols:cols + 128] = v_r.astype(BF16)
        ref[b, at:at + size, lanes + cols:lanes + cols + 128] = (-v_i).astype(BF16)

    for g in range(groups):
        b, l = g // gpb, g % gpb
        f_r, f_i = row(1, b)
        cols = slice(l // per * 128, l // per * 128 + 128)
        c_r, c_i = cmul(spread(cr_v[g], g), spread(ci_v[g], g), f_r[:, cols], f_i[:, cols])
        gain_v[core, 0, g], gain_v[core, 1, g] = c_r, c_i
        place(mats_v, b, l, c_r, c_i)
    out_gain.start()
    for c in out_w:
        c.start()

    r0, r1 = iota((rows, rows), 0), iota((rows, rows), 1)
    shuffle = jnp.where(r1 == (r0 % chunks) * length + r0 // chunks, 1.0, 0.0).astype(BF16)
    back = jnp.where(r1 == (r0 % length) * chunks + r0 // length, 1.0, 0.0).astype(BF16)
    xp_v[...] = jnp.dot(shuffle, x_v[...], preferred_element_type=F32).astype(BF16)
    crow = iota((chunks, lanes), 0)

    def shift(value, s):
        return jnp.where(crow >= s, pltpu.roll(value, s, 0), 0.0)

    def respond(b):
        out = jnp.dot(xp_v[:, b * 128:(b + 1) * 128], bmat_v[b, 128:], preferred_element_type=F32)
        zr_v[b] = out[:, :lanes]
        zi_v[b] = out[:, lanes:]
        a_r, a_i = power(1, b)
        z_r, z_i = zr_v[b, :chunks, :], zi_v[b, :chunks, :]
        for o in range(1, length):
            here = pl.ds(o * chunks, chunks)
            p_r, p_i = cmul(a_r, a_i, z_r, z_i)
            z_r, z_i = p_r + zr_v[b, here, :], p_i + zi_v[b, here, :]
            zr_v[b, here, :] = z_r
            zi_v[b, here, :] = z_i
        s = 1
        while s < chunks:
            m_r, m_i = cmul(*power(length * s, b), shift(z_r, s), shift(z_i, s))
            z_r, z_i = z_r + m_r, z_i + m_i
            s *= 2
        w_r, w_i = shift(z_r, 1), shift(z_i, 1)
        for o in range(length):
            here = pl.ds(o * chunks, chunks)
            w_r, w_i = cmul(a_r, a_i, w_r, w_i)
            zcat_v[b, here, :lanes] = (zr_v[b, here, :] + w_r).astype(BF16)
            zcat_v[b, here, lanes:] = (zi_v[b, here, :] + w_i).astype(BF16)
        col = pl.ds(b * 128, 128)
        out = nt_dot(zcat_v[b], mats_v[b])
        high = out.astype(BF16)
        low = (out - high.astype(F32)).astype(BF16)
        turned = jnp.dot(back, jnp.concatenate([high, low], axis=1), preferred_element_type=F32)
        resp_v[:, col] = turned[:, :128] + turned[:, 128:] + sk_v[:, col] * x_v[:, col].astype(F32)

    def carry_powers(i, which):
        each = [(b, power(8, b, i)) for b in which]
        value = [cmul(*power(1, b, i), *eight(b, False, i)) for b in which]
        for o in range(half // 16):
            here = pl.ds(o * 16, 16)
            after = [cmul(*e, *v) for (_, e), v in zip(each, value)]
            for (b, _), v, n in zip(each, value, after):
                wcat_v[i, b, here, :lanes] = jnp.concatenate([v[0], n[0]], axis=0).astype(BF16)
                wcat_v[i, b, here, lanes:] = jnp.concatenate([v[1], n[1]], axis=0).astype(BF16)
            value = [cmul(*e, *n) for (_, e), n in zip(each, after)]

    def powers(tab, count, a_r, a_i):
        p_r, p_i = jnp.ones((span, wide), F32), jnp.zeros((span, wide), F32)
        for i in range(count):
            tab[i] = jnp.zeros((2 * span, wide), F32)
            tab[count + i, :span], tab[count + i, span:] = p_r, p_i
            p_r, p_i = cmul(p_r, p_i, a_r, a_i)
        return p_r, p_i

    def weight(tab, at, v_r, v_i):
        return cmul(tab[at, :span], tab[at, span:], v_r, v_i)

    def collect(stage, tab, own_r, own_i, receive):
        at, count, _ = lines[stage]
        t_r, t_i = weight(tab, count + count - 1 - at, own_r, own_i)
        p_r = p_i = jnp.zeros((span, wide), F32)
        for k in near_first(count):
            other, v_r, v_i = receive(k)
            m_r, m_i = weight(tab, count + count - 1 - other, v_r, v_i)
            t_r, t_i = t_r + m_r, t_i + m_i
            m_r, m_i = weight(tab, count + at - 1 - other, v_r, v_i)
            p_r, p_i = p_r + m_r, p_i + m_i
        return t_r, t_i, p_r, p_i

    respond(0)
    got_par.wait_recv()

    @pl.when(core == lead)
    def _():
        ax_r, ax_i = powers(tab_x, nx, *pair(1 + squares))
        ay_r, ay_i = powers(tab_y, ny, ax_r, ax_i)
        sum_v[4], sum_v[5] = ay_r, ay_i
        _, own_r, own_i = from_row(0)
        t_r, t_i, p_r, p_i = collect(0, tab_x, own_r, own_i, from_row)
        row_v[:span], row_v[span:] = t_r.astype(BF16), t_i.astype(BF16)
        for k in reversed(near_first(ny)):
            along(1, k).start()
        sum_v[0], sum_v[1], sum_v[2], sum_v[3] = t_r, t_i, p_r, p_i

    for b in range(1, blocks - 1):
        respond(b)
    for b in range(0, blocks, 2):
        carry_powers(core, (b, b + 1))

    @pl.when(core == lead)
    def _():
        t_r, t_i, y_r, y_i = collect(1, tab_y, sum_v[0], sum_v[1], functools.partial(from_line, 1))
        plane_v[:span], plane_v[span:] = t_r.astype(BF16), t_i.astype(BF16)

        @pl.loop(z + 1, nz)
        def _(d):
            pl.semaphore_wait(ready.at[d], 1)
            along(2, d - z).start()

        m_r, m_i = weight(tab_x, nx + x, y_r, y_i)
        sum_v[2], sum_v[3] = sum_v[2] + m_r, sum_v[3] + m_i
        sum_v[0], sum_v[1] = weight(tab_x, nx + x, tab_y[ny + y, :span], tab_y[ny + y, span:])

    respond(blocks - 1)
    out_resp.start()
    both_v[core] = resp_v[rows_of(core), :]
    for b in range(0, blocks, 2):
        carry_powers(other_core, (b, b + 1))

    @pl.when(core == lead)
    def _():
        def gather(k, carry):
            h_r, h_i, p_r, p_i = carry
            _, v_r, v_i = from_line(2, nz - 1 - k)
            m_r, m_i = cmul(p_r, p_i, v_r, v_i)
            return (h_r + m_r, h_i + m_i) + cmul(p_r, p_i, sum_v[4], sum_v[5])

        h_r, h_i, _, _ = lax.fori_loop(0, z, gather, (sum_v[2], sum_v[3], sum_v[0], sum_v[1]))
        pass_v[:span], pass_v[span:] = h_r, h_i
        out_h.start()
        h_v[:span], h_v[span:] = cmul(*pair(late), h_r, h_i)

    @pl.when(core != lead)
    def _():
        out_h.wait_recv()

    got_gain.wait_recv()
    got_resp.wait_recv()
    for i in range(ntp):
        for b in range(blocks):
            for l in range(gpb):
                g, flat = b * gpb + l, l // per * 128
                r, cols = i * tall + b * fold + flat // wide, slice(flat % wide, flat % wide + 128)
                place(keep_v.at[i], b, l, *cmul(
                    gain_v[i, 0, g], gain_v[i, 1, g], h_v[r:r + 1, cols], h_v[span + r:span + r + 1, cols]))
            col = pl.ds(b * 128, 128)
            total = nt_dot(wcat_v[i, b], keep_v[i, b]) + both_v[i, :, col]
            act_v[:, pl.ds(i * depth + b * 128, 128)] = jax.nn.gelu(total).astype(BF16)
    for c in copies[14:]:
        c.wait()
    for c in own_w:
        c.wait()
    for c in got_w:
        c.wait_recv()
    piece = min(512, width)
    for col in [pl.ds(j * piece, piece) for j in range(width // piece)]:
        sums = [bias[:, col] + jnp.dot(act_v[...], w_v[i, :, col], preferred_element_type=F32)
                for i, bias in enumerate((vb_v, gb_v))]
        out_ref[:, col] = (sums[0] * jax.nn.sigmoid(sums[1])).astype(BF16)
    for c in out_w + [out_par, out_gain, out_resp]:
        c.wait_send()
    for k in range(1, nx):
        to_row(k).wait_send()

    @pl.when(core == lead)
    def _():
        out_h.wait_send()
        for k in range(1, ny):
            along(1, k).wait_send()

        @pl.loop(z + 1, nz)
        def _(d):
            along(2, d - z).wait_send()

    @pl.when(core != lead)
    def _():
        to_row(0).wait_send()


def local(nsp, ntp, features, lambda_real, lambda_imag, log_step, input_real, input_imag, real_output,
          imaginary_output, skip_gain, value_weight, gate_weight, value_bias, gate_bias):
    rows, channels = features.shape
    groups, state = lambda_real.shape
    size = input_real.shape[2]
    input_real, input_imag = jnp.swapaxes(input_real, 1, 2), jnp.swapaxes(input_imag, 1, 2)
    width = value_weight.shape[1]
    gpb = 128 // size
    lanes, blocks = gpb * state, groups // gpb
    ring = nz, ny, nx = split_ring(nsp)
    held = (16, 2 * blocks * lanes // 16)
    pairs = (ntp * held[0], held[1])
    half = rows // ntp
    args = (features, lambda_real, lambda_imag, log_step[None], input_real, input_imag, real_output,
            imaginary_output, skip_gain[None], value_weight, gate_weight, value_bias[None], gate_bias[None])
    scratch = [pltpu.VMEM(a.shape, a.dtype) for a in args[:9] + args[11:]]
    scratch += [
        pltpu.VMEM((2, ntp * channels, width), BF16),
        pltpu.VMEM((rows, channels), BF16),
        pltpu.VMEM((blocks, 256, 2 * lanes), BF16),
        pltpu.VMEM((blocks, 128, 2 * lanes), BF16),
        pltpu.VMEM((ntp, blocks, 128, 2 * lanes), BF16),
        pltpu.VMEM((blocks, rows, lanes), F32),
        pltpu.VMEM((blocks, rows, lanes), F32),
        pltpu.VMEM((blocks, rows, 2 * lanes), BF16),
        pltpu.VMEM((ntp, blocks, half, 2 * lanes), BF16),
        pltpu.VMEM((ntp, 2, groups, size, 128), F32),
        pltpu.VMEM((rows, channels), F32),
        pltpu.VMEM((ntp, half, channels), F32),
        pltpu.VMEM((half, ntp * channels), BF16),
        pltpu.VMEM((ntp, 4 + 2 * (rows.bit_length() - 1), 8, held[1]), F32),
        pltpu.VMEM(held, F32),
        pltpu.VMEM((2 * nx,) + pairs, F32),
        pltpu.VMEM((2 * ny,) + pairs, F32),
        pltpu.VMEM((6, pairs[0] // 2, pairs[1]), F32),
        pltpu.VMEM(held, BF16),
        pltpu.VMEM(pairs, BF16),
        pltpu.VMEM(pairs, BF16),
        pltpu.VMEM((nx, ntp) + held, BF16),
        pltpu.VMEM((ny,) + pairs, BF16),
        pltpu.VMEM((nz,) + pairs, BF16),
        pltpu.VMEM(pairs, F32),
        pltpu.VMEM(pairs, F32),
        pltpu.SemaphoreType.DMA((16,)),
        pltpu.SemaphoreType.DMA((2,)),
        pltpu.SemaphoreType.DMA((nx,)),
        pltpu.SemaphoreType.DMA((nx, ntp)),
        pltpu.SemaphoreType.DMA((ny,)),
        pltpu.SemaphoreType.DMA((ny,)),
        pltpu.SemaphoreType.DMA((nz,)),
        pltpu.SemaphoreType.DMA((nz,)),
        pltpu.SemaphoreType.REGULAR((nz,)),
        pltpu.SemaphoreType.DMA((6,)),
        pltpu.SemaphoreType.DMA((6,)),
    ]
    return pl.pallas_call(
        functools.partial(kernel, ring, ntp, (rows, groups, state, size, width)),
        out_shape=pltpu.VMEM((rows // ntp, width), BF16),
        in_specs=[pl.BlockSpec(memory_space=pl.ANY)] * len(args),
        out_specs=pl.BlockSpec(memory_space=pltpu.VMEM),
        scratch_shapes=scratch,
        compiler_params=pltpu.CompilerParams(
            collective_id=0, has_side_effects=True, vmem_limit_bytes=60 * 1024 * 1024),
        name="mixer",
    )(*args)


def solution(mesh):
    in_specs = (
        P("sp", "tp"),
        P("tp", None),
        P("tp", None),
        P("tp"),
        P("tp", None, None),
        P("tp", None, None),
        P("tp", None, None),
        P("tp", None, None),
        P("tp"),
        P("tp", None),
        P("tp", None),
        P(),
        P(),
    )
    out_specs = P(("sp", "tp"), None)
    body = functools.partial(local, mesh.shape["sp"], mesh.shape["tp"])
    return jax.shard_map(body, mesh=mesh, in_specs=in_specs, out_specs=out_specs, check_vma=False)
```

```python
import functools

import jax
import jax.numpy as jnp
from jax import lax
from jax.experimental import pallas as pl
from jax.experimental.pallas import tpu as pltpu
from jax.sharding import PartitionSpec as P

MESH = pl.DeviceIdType.MESH
F32 = jnp.float32
BF16 = jnp.bfloat16


def iota(shape, dim):
    return lax.broadcasted_iota(jnp.int32, shape, dim)


def cmul(ar, ai, br, bi):
    return ar * br - ai * bi, ar * bi + ai * br


def nt_dot(left, right):
    return lax.dot_general(left, right, (((1,), (1,)), ((), ())), preferred_element_type=F32)


def split_ring(nsp):
    nx = min(4, nsp)
    ny = min(8, nsp // nx)
    return nsp // (nx * ny), ny, nx


def near_first(count):
    return sorted(range(1, count), key=lambda k: min(k, count - k))


def kernel(ring, ntp, dims, *refs):
    nz, ny, nx = ring
    rows, groups, state, size, width = dims
    (x_h, lr_h, li_h, ls_h, br_h, bi_h, cr_h, ci_h, sk_h, vw_h, gw_h, vb_h, gb_h, out_ref,
     x_v, ls_v, lam_v, b_v, c_v, sk_v, bias_v, w_v,
     xp_v, bmat_v, mats_v, keep_v, zr_v, zi_v, zcat_v, wcat_v, gain_v, resp_v, both_v, act_v,
     par_v, fin_v, tab_x, tab_y, sum_v, end_v, row_v, plane_v, recv_x, recv_y, recv_z, h_v, pass_v,
     sems, got_sems, ready) = refs
    me = lax.axis_index("sp")
    core = lax.axis_index("tp")
    other_core = 1 - core
    x, y, z = lax.rem(me, nx), lax.rem(me // nx, ny), me // (nx * ny)
    gpb = 128 // size
    lanes = gpb * state
    blocks = groups // gpb
    chunks = 16
    length = rows // chunks
    half = rows // ntp
    tall, wide = fin_v.shape[0] // 2, fin_v.shape[1]
    span = ntp * tall
    lead = ntp - 1
    fold = lanes // wide
    per = 128 // state

    (s_step, s_lam, s_x, s_b, s_c, s_skip, s_bias, s_w, s_h) = (sems.at[i] for i in range(9))
    (g_x, g_y, g_z, g_par, g_gain, g_resp, g_h, g_w0, g_w1) = (got_sems.at[i] for i in range(9))

    def settle(ref, sem):
        pltpu.make_async_copy(ref, ref, sem).wait()

    quarter = rows // 4
    moves = [(ls_h, ls_v, s_step), (lr_h, lam_v.at[0], s_lam), (li_h, lam_v.at[1], s_lam)]
    moves += [(x_h.at[pl.ds(i * quarter, quarter)], x_v.at[pl.ds(i * quarter, quarter)], s_x) for i in range(4)]
    moves += [(br_h, b_v.at[0], s_b), (bi_h, b_v.at[1], s_b), (cr_h, c_v.at[0], s_c), (ci_h, c_v.at[1], s_c)]
    moves += [(sk_h, sk_v, s_skip), (vb_h, bias_v.at[0], s_bias), (gb_h, bias_v.at[1], s_bias)]
    for src, dst, sem in moves:
        pltpu.make_async_copy(src, dst, sem).start()
    depth = vw_h.shape[0]

    def place_of(who):
        return pl.ds(pl.multiple_of(who * depth, depth), depth)

    def rows_of(who):
        return pl.ds(pl.multiple_of(who * half, half), half)

    weights = (vw_h, gw_h)

    def across(src, dst, sent, got):
        return pltpu.make_async_remote_copy(
            src_ref=src, dst_ref=dst, send_sem=sent, recv_sem=got,
            device_id=(me, other_core), device_id_type=MESH)

    wcols = [pl.ds(i * (width // 2), width // 2) for i in range(2)]
    out_w = [[across(s.at[:, cols], w_v.at[i, place_of(core), cols], s_c, got) for i, s in enumerate(weights)]
             for cols, got in zip(wcols, (g_w0, g_w1))]
    out_par, got_par = (across(par_v.at[i], par_v.at[i], s_lam, g_par) for i in (core, other_core))
    out_gain, got_gain = (across(gain_v.at[i], gain_v.at[i], s_b, g_gain) for i in (core, other_core))
    out_resp = across(resp_v.at[rows_of(other_core)], both_v.at[core], s_bias, g_resp)
    got_resp = across(resp_v.at[rows_of(other_core)], both_v.at[other_core], s_bias, g_resp)
    out_h = across(pass_v, h_v, s_h, g_h)

    barrier = pltpu.get_barrier_semaphore()

    def hello(device):
        pl.semaphore_signal(barrier, inc=1, device_id=device, device_id_type=MESH)

    def peer(at, count, stride, k):
        other = lax.rem(at + k, count)
        return other, me + (other - at) * stride

    hello((me, other_core))
    lines = ((x, nx, 1), (y, ny, nx), (z, nz, nx * ny))

    @pl.when(core == lead)
    def _():
        for k in range(1, nx):
            for i in range(ntp):
                hello((peer(*lines[0], k)[1], i))
        for k in range(1, ny):
            hello((peer(*lines[1], k)[1], lead))

        @pl.loop(z + 1, nz)
        def _(d):
            hello((peer(*lines[2], d - z)[1], lead))

    bmat_v[...] = jnp.zeros_like(bmat_v)
    pair_mask = [iota((size, 128), 1) // state == i for i in range(per)]

    def spread(value, g):
        return jnp.where(pair_mask[g % per], jnp.concatenate([value] * per, axis=1), 0.0)

    settle(ls_v, s_step)
    settle(lam_v, s_lam)
    eye = iota((groups, groups), 0) == iota((groups, groups), 1)
    step = jnp.exp(jnp.sum(jnp.where(eye, ls_v[...], 0.0), axis=1, keepdims=True))
    lam_r, lam_i = lam_v[0], lam_v[1]
    mag = jnp.exp(lam_r * step)
    phase = lam_i * step
    t_r, t_i = mag * jnp.cos(phase), mag * jnp.sin(phase)
    den = lam_r * lam_r + lam_i * lam_i
    n_r = t_r - 1.0
    f_r = (n_r * lam_r + t_i * lam_i) / den
    f_i = (t_i * lam_r - n_r * lam_i) / den

    row8, lane8 = iota((gpb, 128), 0), iota((gpb, 128), 1)

    def hold(at, value):
        for b in range(blocks):
            dup = jnp.concatenate([value[b * gpb:(b + 1) * gpb]] * per, axis=1)
            for j in range(gpb // per):
                tile = jnp.sum(jnp.where(row8 == per * j + lane8 // state, dup, 0.0), axis=0, keepdims=True)
                flat = j * 128
                r, c = b * fold + flat // wide, flat % wide
                par_v[core, at, r:r + 1, c:c + 128] = tile

    hold(0, t_r)
    hold(1, t_i)
    hold(2, f_r)
    hold(3, f_i)

    q_r, q_i = par_v[core, 0], par_v[core, 1]
    squares = rows.bit_length() - 1
    for k in range(squares):
        q_r, q_i = cmul(q_r, q_i, q_r, q_i)
        par_v[core, 4 + 2 * k] = q_r
        par_v[core, 5 + 2 * k] = q_i

    def row(k, b, who=core):
        return [jnp.concatenate(
            [par_v[who, 2 * k + i, b * fold + u:b * fold + u + 1] for u in range(fold)], axis=1) for i in range(2)]

    def power(exponent, b, who=core):
        return row(0 if exponent == 1 else exponent.bit_length(), b, who)

    def pair(k):
        return [jnp.concatenate([par_v[i, 2 * k + j] for i in range(ntp)], axis=0) for j in range(2)]

    row_b = iota((8, lanes), 0)

    def eight(b, flip, who=core):
        count = 7 - row_b if flip else row_b
        v_r, v_i = jnp.ones((8, lanes), F32), jnp.zeros((8, lanes), F32)
        for k in range(3):
            bit = (count // (1 << k)) % 2 == 1
            s_r, s_i = power(1 << k, b, who)
            v_r, v_i = cmul(v_r, v_i, jnp.where(bit, s_r, 1.0), jnp.where(bit, s_i, 0.0))
        return v_r, v_i

    settle(x_v, s_x)
    settle(b_v, s_b)
    late = 1 + (half.bit_length() - 1)
    for g in range(groups):
        b, l = g // gpb, g % gpb
        at, cols = l * size, l // per * 128
        lane = slice(cols, cols + 128)
        b_r, b_i = spread(b_v[0, g], g), spread(b_v[1, g], g)
        e_r, e_i = row(late, b)
        m_r, m_i = cmul(b_r, b_i, e_r[:, lane], e_i[:, lane])
        for base, v_r, v_i in ((0, m_r, m_i), (128, b_r, b_i)):
            bmat_v[b, base + at:base + at + size, cols:cols + 128] = v_r.astype(BF16)
            bmat_v[b, base + at:base + at + size, lanes + cols:lanes + cols + 128] = v_i.astype(BF16)

    for b in range(blocks):
        cols = slice(b * 128, (b + 1) * 128)
        both = jnp.concatenate([x_v[:half, cols], x_v[half:, cols]], axis=1)
        out = jnp.dot(both, bmat_v[b], preferred_element_type=F32)
        e_r, e_i = power(8, b)
        z_r, z_i = out[:8, :lanes], out[:8, lanes:]
        for k in range(1, half // 8):
            p_r, p_i = cmul(e_r, e_i, z_r, z_i)
            z_r, z_i = p_r + out[8 * k:8 * k + 8, :lanes], p_i + out[8 * k:8 * k + 8, lanes:]
        v_r, v_i = cmul(*eight(b, True), z_r, z_i)
        v_r, v_i = jnp.sum(v_r, axis=0, keepdims=True), jnp.sum(v_i, axis=0, keepdims=True)
        for u in range(fold):
            at, cols = b * fold + u, slice(u * wide, (u + 1) * wide)
            fin_v[at:at + 1] = v_r[:, cols]
            fin_v[tall + at:tall + at + 1] = v_i[:, cols]
    end_v[...] = fin_v[...].astype(BF16)

    def to_row(k):
        other, device = peer(*lines[0], k)
        return pltpu.make_async_remote_copy(
            src_ref=end_v, dst_ref=recv_x.at[x * ntp + core], send_sem=s_step, recv_sem=g_x,
            device_id=(device, lead), device_id_type=MESH)

    def along(stage, k):
        at = lines[stage][0]
        other, device = peer(*lines[stage], k)
        message, recv, sent, got = ((), (row_v, recv_y, s_x, g_y), (plane_v, recv_z, s_skip, g_z))[stage]
        return pltpu.make_async_remote_copy(
            src_ref=message, dst_ref=recv.at[at], send_sem=sent, recv_sem=got,
            device_id=(device, lead), device_id_type=MESH)

    def settle_some(ref, sem, count, most):
        for i in range(1, most):
            @pl.when(count == i)
            def _():
                settle(ref.at[pl.ds(0, i)], sem)

    def from_row(k):
        other, device = peer(*lines[0], k)
        parts = [fin_v[...] if k == 0 and i == lead else recv_x[other * ntp + i].astype(F32) for i in range(ntp)]
        return (other, jnp.concatenate([p[:tall] for p in parts], axis=0),
                jnp.concatenate([p[tall:] for p in parts], axis=0))

    def from_line(stage, k):
        other, device = peer(*lines[stage], k)
        value = ((), recv_y, recv_z)[stage][other].astype(F32)
        return other, value[:span], value[span:]

    @pl.when(core == lead)
    def _():
        pl.semaphore_wait(barrier, nx - 1 + ny - 1 + ntp - 1 + z)
        for k in reversed(near_first(nx)):
            to_row(k).start()

        @pl.loop(0, z)
        def _(d):
            pl.semaphore_signal(
                ready.at[z], inc=1, device_id=(peer(*lines[2], d - z + nz)[1], lead), device_id_type=MESH)

    @pl.when(core != lead)
    def _():
        pl.semaphore_wait(barrier, nx - 1 + ntp - 1)
        for k in list(reversed(near_first(nx))) + [0]:
            to_row(k).start()

    out_par.start()
    for i, s in enumerate(weights):
        pltpu.make_async_copy(s, w_v.at[i, place_of(core)], s_w).start()

    mats_v[...] = jnp.zeros_like(mats_v)
    keep_v[...] = jnp.zeros_like(keep_v)
    settle(c_v, s_c)
    settle(sk_v, s_skip)
    settle(bias_v, s_bias)

    def place(ref, b, l, v_r, v_i):
        at, cols = l * size, l // per * 128
        ref[b, at:at + size, cols:cols + 128] = v_r.astype(BF16)
        ref[b, at:at + size, lanes + cols:lanes + cols + 128] = (-v_i).astype(BF16)

    for g in range(groups):
        b, l = g // gpb, g % gpb
        f_r, f_i = row(1, b)
        cols = slice(l // per * 128, l // per * 128 + 128)
        c_r, c_i = cmul(spread(c_v[0, g], g), spread(c_v[1, g], g), f_r[:, cols], f_i[:, cols])
        gain_v[core, 0, g], gain_v[core, 1, g] = c_r, c_i
        place(mats_v, b, l, c_r, c_i)
    out_gain.start()
    for c in out_w[0]:
        c.start()

    @pl.when(core == lead)
    def _():
        for c in out_w[1]:
            c.start()

    r0, r1 = iota((rows, rows), 0), iota((rows, rows), 1)
    shuffle = jnp.where(r1 == (r0 % chunks) * length + r0 // chunks, 1.0, 0.0).astype(BF16)
    back = jnp.where(r1 == (r0 % length) * chunks + r0 // length, 1.0, 0.0).astype(BF16)
    xp_v[...] = jnp.dot(shuffle, x_v[...], preferred_element_type=F32).astype(BF16)
    crow = iota((chunks, lanes), 0)

    def shift(value, s):
        return jnp.where(crow >= s, pltpu.roll(value, s, 0), 0.0)

    def respond(b):
        out = jnp.dot(xp_v[:, b * 128:(b + 1) * 128], bmat_v[b, 128:], preferred_element_type=F32)
        zr_v[b] = out[:, :lanes]
        zi_v[b] = out[:, lanes:]
        a_r, a_i = power(1, b)
        z_r, z_i = zr_v[b, :chunks, :], zi_v[b, :chunks, :]
        for o in range(1, length):
            here = pl.ds(o * chunks, chunks)
            p_r, p_i = cmul(a_r, a_i, z_r, z_i)
            z_r, z_i = p_r + zr_v[b, here, :], p_i + zi_v[b, here, :]
            zr_v[b, here, :] = z_r
            zi_v[b, here, :] = z_i
        s = 1
        while s < chunks:
            m_r, m_i = cmul(*power(length * s, b), shift(z_r, s), shift(z_i, s))
            z_r, z_i = z_r + m_r, z_i + m_i
            s *= 2
        w_r, w_i = shift(z_r, 1), shift(z_i, 1)
        for o in range(length):
            here = pl.ds(o * chunks, chunks)
            w_r, w_i = cmul(a_r, a_i, w_r, w_i)
            zcat_v[b, here, :lanes] = (zr_v[b, here, :] + w_r).astype(BF16)
            zcat_v[b, here, lanes:] = (zi_v[b, here, :] + w_i).astype(BF16)
        col = pl.ds(b * 128, 128)
        out = nt_dot(zcat_v[b], mats_v[b])
        high = out.astype(BF16)
        low = (out - high.astype(F32)).astype(BF16)
        turned = jnp.dot(back, jnp.concatenate([high, low], axis=1), preferred_element_type=F32)
        resp_v[:, col] = turned[:, :128] + turned[:, 128:] + sk_v[:, col] * x_v[:, col].astype(F32)

    def carry_powers(i, which):
        each = [(b, power(8, b, i)) for b in which]
        value = [cmul(*power(1, b, i), *eight(b, False, i)) for b in which]
        for o in range(half // 16):
            here = pl.ds(o * 16, 16)
            after = [cmul(*e, *v) for (_, e), v in zip(each, value)]
            for (b, _), v, n in zip(each, value, after):
                wcat_v[i, b, here, :lanes] = jnp.concatenate([v[0], n[0]], axis=0).astype(BF16)
                wcat_v[i, b, here, lanes:] = jnp.concatenate([v[1], n[1]], axis=0).astype(BF16)
            value = [cmul(*e, *n) for (_, e), n in zip(each, after)]

    def powers(tab, count, a_r, a_i):
        p_r, p_i = jnp.ones((span, wide), F32), jnp.zeros((span, wide), F32)
        for i in range(count):
            tab[i] = jnp.zeros((2 * span, wide), F32)
            tab[count + i, :span], tab[count + i, span:] = p_r, p_i
            p_r, p_i = cmul(p_r, p_i, a_r, a_i)
        return p_r, p_i

    def weight(tab, at, v_r, v_i):
        return cmul(tab[at, :span], tab[at, span:], v_r, v_i)

    def collect(stage, tab, own_r, own_i, receive):
        at, count, _ = lines[stage]
        t_r, t_i = weight(tab, count + count - 1 - at, own_r, own_i)
        p_r = p_i = jnp.zeros((span, wide), F32)
        for k in near_first(count):
            other, v_r, v_i = receive(k)
            m_r, m_i = weight(tab, count + count - 1 - other, v_r, v_i)
            t_r, t_i = t_r + m_r, t_i + m_i
            m_r, m_i = weight(tab, count + at - 1 - other, v_r, v_i)
            p_r, p_i = p_r + m_r, p_i + m_i
        return t_r, t_i, p_r, p_i

    respond(0)
    got_par.wait_recv()

    @pl.when(core == lead)
    def _():
        ax_r, ax_i = powers(tab_x, nx, *pair(1 + squares))
        ay_r, ay_i = powers(tab_y, ny, ax_r, ax_i)
        sum_v[4], sum_v[5] = ay_r, ay_i
        settle(recv_x.at[pl.ds(0, nx * ntp - 1)], g_x)
        _, own_r, own_i = from_row(0)
        t_r, t_i, p_r, p_i = collect(0, tab_x, own_r, own_i, from_row)
        row_v[:span], row_v[span:] = t_r.astype(BF16), t_i.astype(BF16)
        for k in reversed(near_first(ny)):
            along(1, k).start()
        sum_v[0], sum_v[1], sum_v[2], sum_v[3] = t_r, t_i, p_r, p_i

    for b in range(1, blocks - 1):
        respond(b)
    for b in range(0, blocks, 2):
        carry_powers(core, (b, b + 1))

    @pl.when(core == lead)
    def _():
        settle(recv_y.at[pl.ds(0, ny - 1)], g_y)
        t_r, t_i, y_r, y_i = collect(1, tab_y, sum_v[0], sum_v[1], functools.partial(from_line, 1))
        plane_v[:span], plane_v[span:] = t_r.astype(BF16), t_i.astype(BF16)

        @pl.loop(z + 1, nz)
        def _(d):
            pl.semaphore_wait(ready.at[d], 1)
            along(2, d - z).start()

        m_r, m_i = weight(tab_x, nx + x, y_r, y_i)
        sum_v[2], sum_v[3] = sum_v[2] + m_r, sum_v[3] + m_i
        sum_v[0], sum_v[1] = weight(tab_x, nx + x, tab_y[ny + y, :span], tab_y[ny + y, span:])

    def hand_on(h_r, h_i):
        pass_v[:span], pass_v[span:] = h_r, h_i
        out_h.start()
        h_v[:span], h_v[span:] = cmul(*pair(late), h_r, h_i)

    @pl.when((core == lead) & (z == 0))
    def _():
        hand_on(sum_v[2], sum_v[3])

    respond(blocks - 1)
    out_resp.start()

    @pl.when(core != lead)
    def _():
        for c in out_w[1]:
            c.start()

    both_v[core] = resp_v[rows_of(core), :]
    for b in range(0, blocks, 2):
        carry_powers(other_core, (b, b + 1))

    @pl.when((core == lead) & (z > 0))
    def _():
        settle_some(recv_z, g_z, z, nz)

        def gather(k, carry):
            h_r, h_i, p_r, p_i = carry
            _, v_r, v_i = from_line(2, nz - 1 - k)
            m_r, m_i = cmul(p_r, p_i, v_r, v_i)
            return (h_r + m_r, h_i + m_i) + cmul(p_r, p_i, sum_v[4], sum_v[5])

        h_r, h_i, _, _ = lax.fori_loop(0, z, gather, (sum_v[2], sum_v[3], sum_v[0], sum_v[1]))
        hand_on(h_r, h_i)

    @pl.when(core != lead)
    def _():
        out_h.wait_recv()

    got_gain.wait_recv()
    got_resp.wait_recv()
    for i in range(ntp):
        for b in range(blocks):
            for l in range(gpb):
                g, flat = b * gpb + l, l // per * 128
                r, cols = i * tall + b * fold + flat // wide, slice(flat % wide, flat % wide + 128)
                place(keep_v.at[i], b, l, *cmul(
                    gain_v[i, 0, g], gain_v[i, 1, g], h_v[r:r + 1, cols], h_v[span + r:span + r + 1, cols]))
            col = pl.ds(b * 128, 128)
            total = nt_dot(wcat_v[i, b], keep_v[i, b]) + both_v[i, :, col]
            act_v[:, pl.ds(i * depth + b * 128, 128)] = jax.nn.gelu(total).astype(BF16)
    settle(w_v.at[:, place_of(core)], s_w)
    settle(w_v.at[:, place_of(other_core), wcols[0]], g_w0)
    piece = min(512, width)
    for j in range(width // piece):
        col = pl.ds(j * piece, piece)
        if j * piece == width // 2:
            settle(w_v.at[:, place_of(other_core), wcols[1]], g_w1)
        sums = [bias_v[i, :, col] + jnp.dot(act_v[...], w_v[i, :, col], preferred_element_type=F32) for i in range(2)]
        out_ref[:, col] = (sums[0] * jax.nn.sigmoid(sums[1])).astype(BF16)
    settle(w_v.at[:, place_of(core)], s_c)
    for c in (out_par, out_gain, out_resp):
        c.wait_send()

    @pl.when(core == lead)
    def _():
        settle(recv_x.at[pl.ds(0, nx - 1)], s_step)
        out_h.wait_send()
        settle(recv_y.at[pl.ds(0, ny - 1)], s_x)
        settle_some(recv_z, s_skip, nz - 1 - z, nz)

    @pl.when(core != lead)
    def _():
        settle(recv_x.at[pl.ds(0, nx)], s_step)


def local(nsp, ntp, features, lambda_real, lambda_imag, log_step, input_real, input_imag, real_output,
          imaginary_output, skip_gain, value_weight, gate_weight, value_bias, gate_bias):
    rows, channels = features.shape
    groups, state = lambda_real.shape
    size = input_real.shape[2]
    input_real, input_imag = jnp.swapaxes(input_real, 1, 2), jnp.swapaxes(input_imag, 1, 2)
    width = value_weight.shape[1]
    gpb = 128 // size
    lanes, blocks = gpb * state, groups // gpb
    ring = nz, ny, nx = split_ring(nsp)
    held = (16, 2 * blocks * lanes // 16)
    pairs = (ntp * held[0], held[1])
    half = rows // ntp
    args = (features, lambda_real, lambda_imag, log_step[None], input_real, input_imag, real_output,
            imaginary_output, skip_gain[None], value_weight, gate_weight, value_bias[None], gate_bias[None])
    scratch = [
        pltpu.VMEM(features.shape, BF16),
        pltpu.VMEM((1, groups), F32),
        pltpu.VMEM((2, groups, state), F32),
        pltpu.VMEM((2, groups, size, state), F32),
        pltpu.VMEM((2, groups, size, state), F32),
        pltpu.VMEM((1, channels), F32),
        pltpu.VMEM((2, 1, width), F32),
    ]
    scratch += [
        pltpu.VMEM((2, ntp * channels, width), BF16),
        pltpu.VMEM((rows, channels), BF16),
        pltpu.VMEM((blocks, 256, 2 * lanes), BF16),
        pltpu.VMEM((blocks, 128, 2 * lanes), BF16),
        pltpu.VMEM((ntp, blocks, 128, 2 * lanes), BF16),
        pltpu.VMEM((blocks, rows, lanes), F32),
        pltpu.VMEM((blocks, rows, lanes), F32),
        pltpu.VMEM((blocks, rows, 2 * lanes), BF16),
        pltpu.VMEM((ntp, blocks, half, 2 * lanes), BF16),
        pltpu.VMEM((ntp, 2, groups, size, 128), F32),
        pltpu.VMEM((rows, channels), F32),
        pltpu.VMEM((ntp, half, channels), F32),
        pltpu.VMEM((half, ntp * channels), BF16),
        pltpu.VMEM((ntp, 4 + 2 * (rows.bit_length() - 1), 8, held[1]), F32),
        pltpu.VMEM(held, F32),
        pltpu.VMEM((2 * nx,) + pairs, F32),
        pltpu.VMEM((2 * ny,) + pairs, F32),
        pltpu.VMEM((6, pairs[0] // 2, pairs[1]), F32),
        pltpu.VMEM(held, BF16),
        pltpu.VMEM(pairs, BF16),
        pltpu.VMEM(pairs, BF16),
        pltpu.VMEM((nx * ntp,) + held, BF16),
        pltpu.VMEM((ny,) + pairs, BF16),
        pltpu.VMEM((nz,) + pairs, BF16),
        pltpu.VMEM(pairs, F32),
        pltpu.VMEM(pairs, F32),
        pltpu.SemaphoreType.DMA((9,)),
        pltpu.SemaphoreType.DMA((9,)),
        pltpu.SemaphoreType.REGULAR((nz,)),
    ]
    return pl.pallas_call(
        functools.partial(kernel, ring, ntp, (rows, groups, state, size, width)),
        out_shape=pltpu.VMEM((rows // ntp, width), BF16),
        in_specs=[pl.BlockSpec(memory_space=pl.ANY)] * len(args),
        out_specs=pl.BlockSpec(memory_space=pltpu.VMEM),
        scratch_shapes=scratch,
        compiler_params=pltpu.CompilerParams(
            collective_id=0, has_side_effects=True, vmem_limit_bytes=60 * 1024 * 1024),
        name="mixer",
    )(*args)


def solution(mesh):
    in_specs = (
        P("sp", "tp"),
        P("tp", None),
        P("tp", None),
        P("tp"),
        P("tp", None, None),
        P("tp", None, None),
        P("tp", None, None),
        P("tp", None, None),
        P("tp"),
        P("tp", None),
        P("tp", None),
        P(),
        P(),
    )
    out_specs = P(("sp", "tp"), None)
    body = functools.partial(local, mesh.shape["sp"], mesh.shape["tp"])
    return jax.shard_map(body, mesh=mesh, in_specs=in_specs, out_specs=out_specs, check_vma=False)
```

```python
import functools

import jax
import jax.numpy as jnp
from jax import lax
from jax.experimental import pallas as pl
from jax.experimental.pallas import tpu as pltpu
from jax.sharding import PartitionSpec as P

MESH = pl.DeviceIdType.MESH
F32 = jnp.float32
BF16 = jnp.bfloat16


def iota(shape, dim):
    return lax.broadcasted_iota(jnp.int32, shape, dim)


def cmul(ar, ai, br, bi):
    return ar * br - ai * bi, ar * bi + ai * br


def nt_dot(left, right):
    return lax.dot_general(left, right, (((1,), (1,)), ((), ())), preferred_element_type=F32)


def split_ring(nsp):
    nx = min(4, nsp)
    ny = min(8, nsp // nx)
    return nsp // (nx * ny), ny, nx


def near_first(count):
    return sorted(range(1, count), key=lambda k: min(k, count - k))


def kernel(ring, ntp, dims, *refs):
    nz, ny, nx = ring
    rows, groups, state, size, width = dims
    (x_h, lr_h, li_h, ls_h, br_h, bi_h, cr_h, ci_h, sk_h, vw_h, gw_h, vb_h, gb_h, out_ref,
     x_v, ls_v, lam_v, b_v, c_v, sk_v, bias_v, w_v,
     xp_v, bmat_v, mats_v, keep_v, zr_v, zi_v, zcat_v, wcat_v, gain_v, resp_v, both_v, act_v,
     par_v, fin_v, tab_x, tab_y, tab_z, sum_v, end_v, row_v, plane_v, recv_x, recv_y, recv_z, h_v, pass_v,
     sems, got_sems, ready) = refs
    me = lax.axis_index("sp")
    core = lax.axis_index("tp")
    other_core = 1 - core
    x, y, z = lax.rem(me, nx), lax.rem(me // nx, ny), me // (nx * ny)
    gpb = 128 // size
    lanes = gpb * state
    blocks = groups // gpb
    chunks = 16
    length = rows // chunks
    half = rows // ntp
    tall, wide = fin_v.shape[0] // 2, fin_v.shape[1]
    span = ntp * tall
    lead = ntp - 1
    fold = lanes // wide
    per = 128 // state

    (s_step, s_lam, s_x, s_b, s_c, s_skip, s_bias, s_w, s_h) = (sems.at[i] for i in range(9))
    (g_x, g_y, g_z, g_par, g_gain, g_resp, g_h, g_w) = (got_sems.at[i] for i in range(8))

    def settle(ref, sem):
        pltpu.make_async_copy(ref, ref, sem).wait()

    quarter = rows // 4
    moves = [(ls_h, ls_v, s_step), (lr_h, lam_v.at[0], s_lam), (li_h, lam_v.at[1], s_lam)]
    moves += [(x_h.at[pl.ds(i * quarter, quarter)], x_v.at[pl.ds(i * quarter, quarter)], s_x) for i in range(4)]
    moves += [(br_h, b_v.at[0], s_b), (bi_h, b_v.at[1], s_b)]
    later = [(cr_h, c_v.at[0], s_c), (ci_h, c_v.at[1], s_c), (sk_h, sk_v, s_skip)]
    later += [(vb_h, bias_v.at[0], s_bias), (gb_h, bias_v.at[1], s_bias)]
    for src, dst, sem in moves:
        pltpu.make_async_copy(src, dst, sem).start()
    depth = vw_h.shape[0]

    def place_of(who):
        return pl.ds(pl.multiple_of(who * depth, depth), depth)

    def rows_of(who):
        return pl.ds(pl.multiple_of(who * half, half), half)

    weights = (vw_h, gw_h)

    def across(src, dst, sent, got):
        return pltpu.make_async_remote_copy(
            src_ref=src, dst_ref=dst, send_sem=sent, recv_sem=got,
            device_id=(me, other_core), device_id_type=MESH)

    first = width // 4 * 3
    wcols = [pl.ds(0, first), pl.ds(first, width - first)]
    out_w = [[across(s.at[:, cols], w_v.at[i, place_of(core), cols], s_c, g_w) for i, s in enumerate(weights)]
             for cols in wcols]
    out_par, got_par = (across(par_v.at[i], par_v.at[i], s_lam, g_par) for i in (core, other_core))
    out_gain, got_gain = (across(gain_v.at[i], gain_v.at[i], s_b, g_gain) for i in (core, other_core))
    out_resp = across(resp_v.at[rows_of(other_core)], both_v.at[core], s_bias, g_resp)
    got_resp = across(resp_v.at[rows_of(other_core)], both_v.at[other_core], s_bias, g_resp)
    out_h = across(pass_v, h_v, s_h, g_h)

    barrier = pltpu.get_barrier_semaphore()

    def hello(device):
        pl.semaphore_signal(barrier, inc=1, device_id=device, device_id_type=MESH)

    def peer(at, count, stride, k):
        other = lax.rem(at + k, count)
        return other, me + (other - at) * stride

    hello((me, other_core))
    lines = ((x, nx, 1), (y, ny, nx), (z, nz, nx * ny))

    @pl.when(core == lead)
    def _():
        for k in range(1, nx):
            for i in range(ntp):
                hello((peer(*lines[0], k)[1], i))
        for k in range(1, ny):
            hello((peer(*lines[1], k)[1], lead))

        @pl.loop(z + 1, nz)
        def _(d):
            hello((peer(*lines[2], d - z)[1], lead))

    bmat_v[...] = jnp.zeros_like(bmat_v)
    pair_mask = [iota((size, 128), 1) // state == i for i in range(per)]

    def spread(value, g):
        return jnp.where(pair_mask[g % per], jnp.concatenate([value] * per, axis=1), 0.0)

    settle(ls_v, s_step)
    settle(lam_v, s_lam)
    eye = iota((groups, groups), 0) == iota((groups, groups), 1)
    step = jnp.exp(jnp.sum(jnp.where(eye, ls_v[...], 0.0), axis=1, keepdims=True))
    lam_r, lam_i = lam_v[0], lam_v[1]
    mag = jnp.exp(lam_r * step)
    phase = lam_i * step
    t_r, t_i = mag * jnp.cos(phase), mag * jnp.sin(phase)
    den = lam_r * lam_r + lam_i * lam_i
    n_r = t_r - 1.0
    f_r = (n_r * lam_r + t_i * lam_i) / den
    f_i = (t_i * lam_r - n_r * lam_i) / den

    row8, lane8 = iota((gpb, 128), 0), iota((gpb, 128), 1)

    def hold(at, value):
        for b in range(blocks):
            dup = jnp.concatenate([value[b * gpb:(b + 1) * gpb]] * per, axis=1)
            for j in range(gpb // per):
                tile = jnp.sum(jnp.where(row8 == per * j + lane8 // state, dup, 0.0), axis=0, keepdims=True)
                flat = j * 128
                r, c = b * fold + flat // wide, flat % wide
                par_v[core, at, r:r + 1, c:c + 128] = tile

    hold(0, t_r)
    hold(1, t_i)
    hold(2, f_r)
    hold(3, f_i)

    q_r, q_i = par_v[core, 0], par_v[core, 1]
    squares = rows.bit_length() - 1
    for k in range(squares):
        q_r, q_i = cmul(q_r, q_i, q_r, q_i)
        par_v[core, 4 + 2 * k] = q_r
        par_v[core, 5 + 2 * k] = q_i

    def row(k, b, who=core):
        return [jnp.concatenate(
            [par_v[who, 2 * k + i, b * fold + u:b * fold + u + 1] for u in range(fold)], axis=1) for i in range(2)]

    def power(exponent, b, who=core):
        return row(0 if exponent == 1 else exponent.bit_length(), b, who)

    def pair(k):
        return [jnp.concatenate([par_v[i, 2 * k + j] for i in range(ntp)], axis=0) for j in range(2)]

    row_b = iota((8, lanes), 0)

    def eight(b, flip, who=core):
        count = 7 - row_b if flip else row_b
        v_r, v_i = jnp.ones((8, lanes), F32), jnp.zeros((8, lanes), F32)
        for k in range(3):
            bit = (count // (1 << k)) % 2 == 1
            s_r, s_i = power(1 << k, b, who)
            v_r, v_i = cmul(v_r, v_i, jnp.where(bit, s_r, 1.0), jnp.where(bit, s_i, 0.0))
        return v_r, v_i

    settle(x_v, s_x)
    settle(b_v, s_b)
    for src, dst, sem in later:
        pltpu.make_async_copy(src, dst, sem).start()
    late = 1 + (half.bit_length() - 1)
    for g in range(groups):
        b, l = g // gpb, g % gpb
        at, cols = l * size, l // per * 128
        lane = slice(cols, cols + 128)
        b_r, b_i = spread(b_v[0, g], g), spread(b_v[1, g], g)
        e_r, e_i = row(late, b)
        m_r, m_i = cmul(b_r, b_i, e_r[:, lane], e_i[:, lane])
        for base, v_r, v_i in ((0, m_r, m_i), (128, b_r, b_i)):
            bmat_v[b, base + at:base + at + size, cols:cols + 128] = v_r.astype(BF16)
            bmat_v[b, base + at:base + at + size, lanes + cols:lanes + cols + 128] = v_i.astype(BF16)

    for b in range(blocks):
        cols = slice(b * 128, (b + 1) * 128)
        both = jnp.concatenate([x_v[:half, cols], x_v[half:, cols]], axis=1)
        out = jnp.dot(both, bmat_v[b], preferred_element_type=F32)
        zr_v[b, :half] = out[:, :lanes]
        zi_v[b, :half] = out[:, lanes:]
    for which in [(b, b + 1) for b in range(0, blocks, 2)]:
        each = [power(8, b) for b in which]
        value = [(zr_v[b, :8], zi_v[b, :8]) for b in which]
        for k in range(1, half // 8):
            here = pl.ds(8 * k, 8)
            moved = [cmul(*e, *v) for e, v in zip(each, value)]
            value = [(m_r + zr_v[b, here], m_i + zi_v[b, here]) for b, (m_r, m_i) in zip(which, moved)]
        for b, v in zip(which, value):
            v_r, v_i = cmul(*eight(b, True), *v)
            v_r, v_i = jnp.sum(v_r, axis=0, keepdims=True), jnp.sum(v_i, axis=0, keepdims=True)
            for u in range(fold):
                at, cols = b * fold + u, slice(u * wide, (u + 1) * wide)
                fin_v[at:at + 1] = v_r[:, cols]
                fin_v[tall + at:tall + at + 1] = v_i[:, cols]
    end_v[...] = fin_v[...].astype(BF16)

    def to_row(k):
        other, device = peer(*lines[0], k)
        return pltpu.make_async_remote_copy(
            src_ref=end_v, dst_ref=recv_x.at[x * ntp + core], send_sem=s_step, recv_sem=g_x,
            device_id=(device, lead), device_id_type=MESH)

    def along(stage, k):
        at = lines[stage][0]
        other, device = peer(*lines[stage], k)
        message, recv, sent, got = ((), (row_v, recv_y, s_x, g_y), (plane_v, recv_z, s_skip, g_z))[stage]
        return pltpu.make_async_remote_copy(
            src_ref=message, dst_ref=recv.at[at], send_sem=sent, recv_sem=got,
            device_id=(device, lead), device_id_type=MESH)

    def settle_some(ref, sem, count, most):
        for i in range(1, most):
            @pl.when(count == i)
            def _():
                settle(ref.at[pl.ds(0, i)], sem)

    def from_row(k):
        other, device = peer(*lines[0], k)
        parts = [fin_v[...] if k == 0 and i == lead else recv_x[other * ntp + i].astype(F32) for i in range(ntp)]
        return (other, jnp.concatenate([p[:tall] for p in parts], axis=0),
                jnp.concatenate([p[tall:] for p in parts], axis=0))

    def from_line(stage, k):
        other, device = peer(*lines[stage], k)
        value = ((), recv_y, recv_z)[stage][other].astype(F32)
        return other, value[:span], value[span:]

    @pl.when(core == lead)
    def _():
        pl.semaphore_wait(barrier, nx - 1 + ny - 1 + ntp - 1 + z)
        for k in reversed(near_first(nx)):
            to_row(k).start()

        @pl.loop(0, z)
        def _(d):
            pl.semaphore_signal(
                ready, inc=1, device_id=(peer(*lines[2], d - z + nz)[1], lead), device_id_type=MESH)

    @pl.when(core != lead)
    def _():
        pl.semaphore_wait(barrier, nx - 1 + ntp - 1)
        for k in list(reversed(near_first(nx))) + [0]:
            to_row(k).start()

    out_par.start()
    for i, s in enumerate(weights):
        pltpu.make_async_copy(s, w_v.at[i, place_of(core)], s_w).start()

    mats_v[...] = jnp.zeros_like(mats_v)
    keep_v[...] = jnp.zeros_like(keep_v)
    settle(c_v, s_c)
    settle(sk_v, s_skip)
    settle(bias_v, s_bias)

    def place(ref, b, l, v_r, v_i):
        at, cols = l * size, l // per * 128
        ref[b, at:at + size, cols:cols + 128] = v_r.astype(BF16)
        ref[b, at:at + size, lanes + cols:lanes + cols + 128] = (-v_i).astype(BF16)

    for g in range(groups):
        b, l = g // gpb, g % gpb
        f_r, f_i = row(1, b)
        cols = slice(l // per * 128, l // per * 128 + 128)
        c_r, c_i = cmul(spread(c_v[0, g], g), spread(c_v[1, g], g), f_r[:, cols], f_i[:, cols])
        gain_v[core, 0, g], gain_v[core, 1, g] = c_r, c_i
        place(mats_v, b, l, c_r, c_i)
    out_gain.start()
    for c in out_w[0]:
        c.start()

    @pl.when(core == lead)
    def _():
        for c in out_w[1]:
            c.start()

    r0, r1 = iota((rows, rows), 0), iota((rows, rows), 1)
    shuffle = jnp.where(r1 == (r0 % chunks) * length + r0 // chunks, 1.0, 0.0).astype(BF16)
    back = jnp.where(r1 == (r0 % length) * chunks + r0 // length, 1.0, 0.0).astype(BF16)
    xp_v[...] = jnp.dot(shuffle, x_v[...], preferred_element_type=F32).astype(BF16)
    crow = iota((chunks, lanes), 0)

    def shift(value, s):
        return jnp.where(crow >= s, pltpu.roll(value, s, 0), 0.0)

    def respond(b):
        out = jnp.dot(xp_v[:, b * 128:(b + 1) * 128], bmat_v[b, 128:], preferred_element_type=F32)
        zr_v[b] = out[:, :lanes]
        zi_v[b] = out[:, lanes:]
        a_r, a_i = power(1, b)
        z_r, z_i = zr_v[b, :chunks, :], zi_v[b, :chunks, :]
        for o in range(1, length):
            here = pl.ds(o * chunks, chunks)
            p_r, p_i = cmul(a_r, a_i, z_r, z_i)
            z_r, z_i = p_r + zr_v[b, here, :], p_i + zi_v[b, here, :]
            zr_v[b, here, :] = z_r
            zi_v[b, here, :] = z_i
        s = 1
        while s < chunks:
            m_r, m_i = cmul(*power(length * s, b), shift(z_r, s), shift(z_i, s))
            z_r, z_i = z_r + m_r, z_i + m_i
            s *= 2
        w_r, w_i = shift(z_r, 1), shift(z_i, 1)
        for o in range(length):
            here = pl.ds(o * chunks, chunks)
            w_r, w_i = cmul(a_r, a_i, w_r, w_i)
            zcat_v[b, here, :lanes] = (zr_v[b, here, :] + w_r).astype(BF16)
            zcat_v[b, here, lanes:] = (zi_v[b, here, :] + w_i).astype(BF16)
        col = pl.ds(b * 128, 128)
        out = nt_dot(zcat_v[b], mats_v[b])
        high = out.astype(BF16)
        low = (out - high.astype(F32)).astype(BF16)
        turned = jnp.dot(back, jnp.concatenate([high, low], axis=1), preferred_element_type=F32)
        resp_v[:, col] = turned[:, :128] + turned[:, 128:] + sk_v[:, col] * x_v[:, col].astype(F32)

    def carry_powers(i, which):
        each = [(b, power(8, b, i)) for b in which]
        value = [cmul(*power(1, b, i), *eight(b, False, i)) for b in which]
        for o in range(half // 16):
            here = pl.ds(o * 16, 16)
            after = [cmul(*e, *v) for (_, e), v in zip(each, value)]
            for (b, _), v, n in zip(each, value, after):
                wcat_v[i, b, here, :lanes] = jnp.concatenate([v[0], n[0]], axis=0).astype(BF16)
                wcat_v[i, b, here, lanes:] = jnp.concatenate([v[1], n[1]], axis=0).astype(BF16)
            value = [cmul(*e, *n) for (_, e), n in zip(each, after)]

    def powers(tab, count, a_r, a_i):
        p_r, p_i = jnp.ones((span, wide), F32), jnp.zeros((span, wide), F32)
        for i in range(count):
            tab[i] = jnp.zeros((2 * span, wide), F32)
            tab[count + i, :span], tab[count + i, span:] = p_r, p_i
            p_r, p_i = cmul(p_r, p_i, a_r, a_i)
        return p_r, p_i

    def weight(tab, at, v_r, v_i):
        return cmul(tab[at, :span], tab[at, span:], v_r, v_i)

    def collect(stage, tab, own_r, own_i, receive):
        at, count, _ = lines[stage]
        t_r, t_i = weight(tab, count + count - 1 - at, own_r, own_i)
        p_r = p_i = jnp.zeros((span, wide), F32)
        for k in near_first(count):
            other, v_r, v_i = receive(k)
            m_r, m_i = weight(tab, count + count - 1 - other, v_r, v_i)
            t_r, t_i = t_r + m_r, t_i + m_i
            m_r, m_i = weight(tab, count + at - 1 - other, v_r, v_i)
            p_r, p_i = p_r + m_r, p_i + m_i
        return t_r, t_i, p_r, p_i

    respond(0)
    got_par.wait_recv()

    @pl.when(core == lead)
    def _():
        ax_r, ax_i = powers(tab_x, nx, *pair(1 + squares))
        ay_r, ay_i = powers(tab_y, ny, ax_r, ax_i)
        sum_v[4], sum_v[5] = ay_r, ay_i
        settle(recv_x.at[pl.ds(0, nx * ntp - 1)], g_x)
        _, own_r, own_i = from_row(0)
        t_r, t_i, p_r, p_i = collect(0, tab_x, own_r, own_i, from_row)
        row_v[:span], row_v[span:] = t_r.astype(BF16), t_i.astype(BF16)
        for k in reversed(near_first(ny)):
            along(1, k).start()
        sum_v[0], sum_v[1], sum_v[2], sum_v[3] = t_r, t_i, p_r, p_i

    for b in range(1, blocks - 1):
        respond(b)
    for b in range(0, blocks, 2):
        carry_powers(core, (b, b + 1))

    respond(blocks - 1)
    out_resp.start()

    @pl.when(core != lead)
    def _():
        for c in out_w[1]:
            c.start()

    both_v[core] = resp_v[rows_of(core), :]
    for b in range(0, blocks, 2):
        carry_powers(other_core, (b, b + 1))

    def hand_on(h_r, h_i):
        pass_v[:span], pass_v[span:] = h_r, h_i
        out_h.start()
        h_v[:span], h_v[span:] = cmul(*pair(late), h_r, h_i)

    @pl.when(core == lead)
    def _():
        s_r, s_i = weight(tab_x, nx + x, tab_y[ny + y, :span], tab_y[ny + y, span:])
        for i in range(nz - 1):
            tab_z[i, :span], tab_z[i, span:] = s_r, s_i
            s_r, s_i = cmul(s_r, s_i, sum_v[4], sum_v[5])
        settle(recv_y.at[pl.ds(0, ny - 1)], g_y)
        t_r, t_i, y_r, y_i = collect(1, tab_y, sum_v[0], sum_v[1], functools.partial(from_line, 1))
        plane_v[:span], plane_v[span:] = t_r.astype(BF16), t_i.astype(BF16)

        @pl.when(z < nz - 1)
        def _():
            pl.semaphore_wait(ready, nz - 1 - z)

        @pl.loop(0, nz - 1 - z)
        def _(i):
            d = jnp.where(z >= nz // 2, nz - 1 - i, z + 1 + i)
            along(2, d - z).start()

        m_r, m_i = weight(tab_x, nx + x, y_r, y_i)
        h_r, h_i = sum_v[2] + m_r, sum_v[3] + m_i
        sum_v[2], sum_v[3] = h_r, h_i

        @pl.when(z == 0)
        def _():
            hand_on(h_r, h_i)

        @pl.when(z > 0)
        def _():
            settle_some(recv_z, g_z, z, nz)

            def gather(k, carry):
                h_r, h_i = carry
                _, v_r, v_i = from_line(2, nz - 1 - k)
                m_r, m_i = weight(tab_z, k, v_r, v_i)
                return h_r + m_r, h_i + m_i

            hand_on(*lax.fori_loop(0, z, gather, (sum_v[2], sum_v[3])))

    @pl.when(core != lead)
    def _():
        out_h.wait_recv()

    got_gain.wait_recv()
    got_resp.wait_recv()
    for i in range(ntp):
        for b in range(blocks):
            for l in range(gpb):
                g, flat = b * gpb + l, l // per * 128
                r, cols = i * tall + b * fold + flat // wide, slice(flat % wide, flat % wide + 128)
                place(keep_v.at[i], b, l, *cmul(
                    gain_v[i, 0, g], gain_v[i, 1, g], h_v[r:r + 1, cols], h_v[span + r:span + r + 1, cols]))
            col = pl.ds(b * 128, 128)
            total = nt_dot(wcat_v[i, b], keep_v[i, b]) + both_v[i, :, col]
            act_v[:, pl.ds(i * depth + b * 128, 128)] = jax.nn.gelu(total).astype(BF16)
    settle(w_v.at[:, place_of(core)], s_w)
    settle(w_v.at[:, place_of(other_core)], g_w)
    piece = min(512, width)
    for j in range(width // piece):
        col = pl.ds(j * piece, piece)
        sums = [bias_v[i, :, col] + jnp.dot(act_v[...], w_v[i, :, col], preferred_element_type=F32) for i in range(2)]
        out_ref[:, col] = (sums[0] * jax.nn.sigmoid(sums[1])).astype(BF16)
    settle(w_v.at[:, place_of(core)], s_c)
    for c in (out_par, out_gain, out_resp):
        c.wait_send()

    @pl.when(core == lead)
    def _():
        settle(recv_x.at[pl.ds(0, nx - 1)], s_step)
        out_h.wait_send()
        settle(recv_y.at[pl.ds(0, ny - 1)], s_x)
        settle_some(recv_z, s_skip, nz - 1 - z, nz)

    @pl.when(core != lead)
    def _():
        settle(recv_x.at[pl.ds(0, nx)], s_step)


def local(nsp, ntp, features, lambda_real, lambda_imag, log_step, input_real, input_imag, real_output,
          imaginary_output, skip_gain, value_weight, gate_weight, value_bias, gate_bias):
    rows, channels = features.shape
    groups, state = lambda_real.shape
    size = input_real.shape[2]
    input_real, input_imag = jnp.swapaxes(input_real, 1, 2), jnp.swapaxes(input_imag, 1, 2)
    width = value_weight.shape[1]
    gpb = 128 // size
    lanes, blocks = gpb * state, groups // gpb
    ring = nz, ny, nx = split_ring(nsp)
    held = (16, 2 * blocks * lanes // 16)
    pairs = (ntp * held[0], held[1])
    half = rows // ntp
    args = (features, lambda_real, lambda_imag, log_step[None], input_real, input_imag, real_output,
            imaginary_output, skip_gain[None], value_weight, gate_weight, value_bias[None], gate_bias[None])
    scratch = [
        pltpu.VMEM(features.shape, BF16),
        pltpu.VMEM((1, groups), F32),
        pltpu.VMEM((2, groups, state), F32),
        pltpu.VMEM((2, groups, size, state), F32),
        pltpu.VMEM((2, groups, size, state), F32),
        pltpu.VMEM((1, channels), F32),
        pltpu.VMEM((2, 1, width), F32),
    ]
    scratch += [
        pltpu.VMEM((2, ntp * channels, width), BF16),
        pltpu.VMEM((rows, channels), BF16),
        pltpu.VMEM((blocks, 256, 2 * lanes), BF16),
        pltpu.VMEM((blocks, 128, 2 * lanes), BF16),
        pltpu.VMEM((ntp, blocks, 128, 2 * lanes), BF16),
        pltpu.VMEM((blocks, rows, lanes), F32),
        pltpu.VMEM((blocks, rows, lanes), F32),
        pltpu.VMEM((blocks, rows, 2 * lanes), BF16),
        pltpu.VMEM((ntp, blocks, half, 2 * lanes), BF16),
        pltpu.VMEM((ntp, 2, groups, size, 128), F32),
        pltpu.VMEM((rows, channels), F32),
        pltpu.VMEM((ntp, half, channels), F32),
        pltpu.VMEM((half, ntp * channels), BF16),
        pltpu.VMEM((ntp, 4 + 2 * (rows.bit_length() - 1), 8, held[1]), F32),
        pltpu.VMEM(held, F32),
        pltpu.VMEM((2 * nx,) + pairs, F32),
        pltpu.VMEM((2 * ny,) + pairs, F32),
        pltpu.VMEM((nz - 1,) + pairs, F32),
        pltpu.VMEM((6, pairs[0] // 2, pairs[1]), F32),
        pltpu.VMEM(held, BF16),
        pltpu.VMEM(pairs, BF16),
        pltpu.VMEM(pairs, BF16),
        pltpu.VMEM((nx * ntp,) + held, BF16),
        pltpu.VMEM((ny,) + pairs, BF16),
        pltpu.VMEM((nz,) + pairs, BF16),
        pltpu.VMEM(pairs, F32),
        pltpu.VMEM(pairs, F32),
        pltpu.SemaphoreType.DMA((9,)),
        pltpu.SemaphoreType.DMA((8,)),
        pltpu.SemaphoreType.REGULAR,
    ]
    return pl.pallas_call(
        functools.partial(kernel, ring, ntp, (rows, groups, state, size, width)),
        out_shape=pltpu.VMEM((rows // ntp, width), BF16),
        in_specs=[pl.BlockSpec(memory_space=pl.ANY)] * len(args),
        out_specs=pl.BlockSpec(memory_space=pltpu.VMEM),
        scratch_shapes=scratch,
        compiler_params=pltpu.CompilerParams(
            collective_id=0, has_side_effects=True, vmem_limit_bytes=60 * 1024 * 1024),
        name="mixer",
    )(*args)


def solution(mesh):
    in_specs = (
        P("sp", "tp"),
        P("tp", None),
        P("tp", None),
        P("tp"),
        P("tp", None, None),
        P("tp", None, None),
        P("tp", None, None),
        P("tp", None, None),
        P("tp"),
        P("tp", None),
        P("tp", None),
        P(),
        P(),
    )
    out_specs = P(("sp", "tp"), None)
    body = functools.partial(local, mesh.shape["sp"], mesh.shape["tp"])
    return jax.shard_map(body, mesh=mesh, in_specs=in_specs, out_specs=out_specs, check_vma=False)
```

```python
import functools

import jax
import jax.numpy as jnp
from jax import lax
from jax.experimental import pallas as pl
from jax.experimental.pallas import tpu as pltpu
from jax.sharding import PartitionSpec as P

MESH = pl.DeviceIdType.MESH
F32 = jnp.float32
BF16 = jnp.bfloat16


def iota(shape, dim):
    return lax.broadcasted_iota(jnp.int32, shape, dim)


def cmul(ar, ai, br, bi):
    return ar * br - ai * bi, ar * bi + ai * br


def nt_dot(left, right):
    return lax.dot_general(left, right, (((1,), (1,)), ((), ())), preferred_element_type=F32)


def split_ring(nsp):
    nx = min(4, nsp)
    ny = min(8, nsp // nx)
    return nsp // (nx * ny), ny, nx


def near_first(count):
    return sorted(range(1, count), key=lambda k: min(k, count - k))


def kernel(ring, ntp, dims, *refs):
    nz, ny, nx = ring
    rows, groups, state, size, width = dims
    (x_h, lr_h, li_h, ls_h, br_h, bi_h, cr_h, ci_h, sk_h, vw_h, gw_h, vb_h, gb_h, out_ref,
     x_v, ls_v, lam_v, b_v, c_v, sk_v, bias_v, w_v,
     xp_v, bmat_v, mats_v, keep_v, zr_v, zi_v, zcat_v, wcat_v, gain_v, resp_v, both_v, act_v,
     par_v, fin_v, tab_x, tab_y, tab_z, sum_v, end_v, row_v, plane_v, recv_x, recv_y, recv_z, h_v, pass_v,
     sems, got_sems, ready) = refs
    me = lax.axis_index("sp")
    core = lax.axis_index("tp")
    other_core = 1 - core
    x, y, z = lax.rem(me, nx), lax.rem(me // nx, ny), me // (nx * ny)
    gpb = 128 // size
    lanes = gpb * state
    blocks = groups // gpb
    chunks = 16
    length = rows // chunks
    half = rows // ntp
    tall, wide = fin_v.shape[0] // 2, fin_v.shape[1]
    span = ntp * tall
    lead = ntp - 1
    fold = lanes // wide
    per = 128 // state

    (s_step, s_lam, s_x, s_b, s_c, s_skip, s_bias, s_w, s_h) = (sems.at[i] for i in range(9))
    (g_x, g_y, g_z, g_par, g_gain, g_resp, g_h, g_w) = (got_sems.at[i] for i in range(8))

    def settle(ref, sem):
        pltpu.make_async_copy(ref, ref, sem).wait()

    quarter = rows // 4
    moves = [(ls_h, ls_v, s_step), (lr_h, lam_v.at[0], s_lam), (li_h, lam_v.at[1], s_lam)]
    moves += [(x_h.at[pl.ds(i * quarter, quarter)], x_v.at[pl.ds(i * quarter, quarter)], s_x) for i in range(4)]
    moves += [(br_h, b_v.at[0], s_b), (bi_h, b_v.at[1], s_b)]
    later = [(cr_h, c_v.at[0], s_c), (ci_h, c_v.at[1], s_c), (sk_h, sk_v, s_skip)]
    later += [(vb_h, bias_v.at[0], s_bias), (gb_h, bias_v.at[1], s_bias)]
    for src, dst, sem in moves:
        pltpu.make_async_copy(src, dst, sem).start()
    depth = vw_h.shape[0]

    def place_of(who):
        return pl.ds(pl.multiple_of(who * depth, depth), depth)

    def rows_of(who):
        return pl.ds(pl.multiple_of(who * half, half), half)

    weights = (vw_h, gw_h)

    def across(src, dst, sent, got):
        return pltpu.make_async_remote_copy(
            src_ref=src, dst_ref=dst, send_sem=sent, recv_sem=got,
            device_id=(me, other_core), device_id_type=MESH)

    first = width // 4 * 3
    wcols = [pl.ds(0, first), pl.ds(first, width - first)]
    out_w = [[across(s.at[:, cols], w_v.at[i, place_of(core), cols], s_c, g_w) for i, s in enumerate(weights)]
             for cols in wcols]
    out_par, got_par = (across(par_v.at[i], par_v.at[i], s_lam, g_par) for i in (core, other_core))
    out_gain, got_gain = (across(gain_v.at[i], gain_v.at[i], s_b, g_gain) for i in (core, other_core))
    out_resp = across(resp_v.at[rows_of(other_core)], both_v.at[core], s_bias, g_resp)
    got_resp = across(resp_v.at[rows_of(other_core)], both_v.at[other_core], s_bias, g_resp)
    out_h = across(pass_v, h_v, s_h, g_h)

    barrier = pltpu.get_barrier_semaphore()

    def hello(device):
        pl.semaphore_signal(barrier, inc=1, device_id=device, device_id_type=MESH)

    def peer(at, count, stride, k):
        other = lax.rem(at + k, count)
        return other, me + (other - at) * stride

    hello((me, other_core))
    lines = ((x, nx, 1), (y, ny, nx), (z, nz, nx * ny))

    @pl.when(core == lead)
    def _():
        for k in range(1, nx):
            for i in range(ntp):
                hello((peer(*lines[0], k)[1], i))
        for k in range(1, ny):
            hello((peer(*lines[1], k)[1], lead))

        @pl.loop(z + 1, nz)
        def _(d):
            hello((peer(*lines[2], d - z)[1], lead))

    bmat_v[...] = jnp.zeros_like(bmat_v)
    pair_mask = [iota((size, 128), 1) // state == i for i in range(per)]

    def spread(value, g):
        return jnp.where(pair_mask[g % per], jnp.concatenate([value] * per, axis=1), 0.0)

    settle(ls_v, s_step)
    settle(lam_v, s_lam)
    eye = iota((groups, groups), 0) == iota((groups, groups), 1)
    step = jnp.exp(jnp.sum(jnp.where(eye, ls_v[...], 0.0), axis=1, keepdims=True))
    lam_r, lam_i = lam_v[0], lam_v[1]
    mag = jnp.exp(lam_r * step)
    phase = lam_i * step
    t_r, t_i = mag * jnp.cos(phase), mag * jnp.sin(phase)
    den = lam_r * lam_r + lam_i * lam_i
    n_r = t_r - 1.0
    f_r = (n_r * lam_r + t_i * lam_i) / den
    f_i = (t_i * lam_r - n_r * lam_i) / den

    row8, lane8 = iota((gpb, 128), 0), iota((gpb, 128), 1)

    def hold(at, value):
        for b in range(blocks):
            dup = jnp.concatenate([value[b * gpb:(b + 1) * gpb]] * per, axis=1)
            for j in range(gpb // per):
                tile = jnp.sum(jnp.where(row8 == per * j + lane8 // state, dup, 0.0), axis=0, keepdims=True)
                flat = j * 128
                r, c = b * fold + flat // wide, flat % wide
                par_v[core, at, r:r + 1, c:c + 128] = tile

    hold(0, t_r)
    hold(1, t_i)
    hold(2, f_r)
    hold(3, f_i)

    q_r, q_i = par_v[core, 0], par_v[core, 1]
    squares = rows.bit_length() - 1
    for k in range(squares):
        q_r, q_i = cmul(q_r, q_i, q_r, q_i)
        par_v[core, 4 + 2 * k] = q_r
        par_v[core, 5 + 2 * k] = q_i

    def row(k, b, who=core):
        return [jnp.concatenate(
            [par_v[who, 2 * k + i, b * fold + u:b * fold + u + 1] for u in range(fold)], axis=1) for i in range(2)]

    def power(exponent, b, who=core):
        return row(0 if exponent == 1 else exponent.bit_length(), b, who)

    def pair(k):
        return [jnp.concatenate([par_v[i, 2 * k + j] for i in range(ntp)], axis=0) for j in range(2)]

    row_b = iota((8, lanes), 0)

    def eight(b, flip, who=core):
        count = 7 - row_b if flip else row_b
        v_r, v_i = jnp.ones((8, lanes), F32), jnp.zeros((8, lanes), F32)
        for k in range(3):
            bit = (count // (1 << k)) % 2 == 1
            s_r, s_i = power(1 << k, b, who)
            v_r, v_i = cmul(v_r, v_i, jnp.where(bit, s_r, 1.0), jnp.where(bit, s_i, 0.0))
        return v_r, v_i

    settle(x_v, s_x)
    settle(b_v, s_b)
    for src, dst, sem in later:
        pltpu.make_async_copy(src, dst, sem).start()
    late = 1 + (half.bit_length() - 1)
    for g in range(groups):
        b, l = g // gpb, g % gpb
        at, cols = l * size, l // per * 128
        lane = slice(cols, cols + 128)
        b_r, b_i = spread(b_v[0, g], g), spread(b_v[1, g], g)
        e_r, e_i = row(late, b)
        m_r, m_i = cmul(b_r, b_i, e_r[:, lane], e_i[:, lane])
        for base, v_r, v_i in ((0, m_r, m_i), (128, b_r, b_i)):
            bmat_v[b, base + at:base + at + size, cols:cols + 128] = v_r.astype(BF16)
            bmat_v[b, base + at:base + at + size, lanes + cols:lanes + cols + 128] = v_i.astype(BF16)

    def fold_halves(b):
        cols = slice(b * 128, (b + 1) * 128)
        both = jnp.concatenate([x_v[:half, cols], x_v[half:, cols]], axis=1)
        out = jnp.dot(both, bmat_v[b], preferred_element_type=F32)
        zr_v[b, :half] = out[:, :lanes]
        zi_v[b, :half] = out[:, lanes:]

    fold_halves(0)
    for b in range(blocks):
        if b + 1 < blocks:
            fold_halves(b + 1)
        e_r, e_i = power(8, b)
        part = half // 2
        value = [(zr_v[b, i * part:i * part + 8], zi_v[b, i * part:i * part + 8]) for i in range(2)]
        for k in range(1, part // 8):
            moved = [cmul(e_r, e_i, *v) for v in value]
            value = [(m_r + zr_v[b, i * part + 8 * k:i * part + 8 * k + 8], m_i + zi_v[b, i * part + 8 * k:i * part + 8 * k + 8])
                     for i, (m_r, m_i) in enumerate(moved)]
        m_r, m_i = cmul(*power(part, b), *value[0])
        v_r, v_i = cmul(*eight(b, True), m_r + value[1][0], m_i + value[1][1])
        v_r, v_i = jnp.sum(v_r, axis=0, keepdims=True), jnp.sum(v_i, axis=0, keepdims=True)
        for u in range(fold):
            at, cols = b * fold + u, slice(u * wide, (u + 1) * wide)
            fin_v[at:at + 1] = v_r[:, cols]
            fin_v[tall + at:tall + at + 1] = v_i[:, cols]
    end_v[...] = fin_v[...].astype(BF16)

    def to_row(k):
        other, device = peer(*lines[0], k)
        return pltpu.make_async_remote_copy(
            src_ref=end_v, dst_ref=recv_x.at[x * ntp + core], send_sem=s_step, recv_sem=g_x,
            device_id=(device, lead), device_id_type=MESH)

    def along(stage, k):
        at = lines[stage][0]
        other, device = peer(*lines[stage], k)
        message, recv, sent, got = ((), (row_v, recv_y, s_x, g_y), (plane_v, recv_z, s_skip, g_z))[stage]
        return pltpu.make_async_remote_copy(
            src_ref=message, dst_ref=recv.at[at], send_sem=sent, recv_sem=got,
            device_id=(device, lead), device_id_type=MESH)

    def settle_some(ref, sem, count, most):
        for i in range(1, most):
            @pl.when(count == i)
            def _():
                settle(ref.at[pl.ds(0, i)], sem)

    def from_row(k):
        other, device = peer(*lines[0], k)
        parts = [fin_v[...] if k == 0 and i == lead else recv_x[other * ntp + i].astype(F32) for i in range(ntp)]
        return (other, jnp.concatenate([p[:tall] for p in parts], axis=0),
                jnp.concatenate([p[tall:] for p in parts], axis=0))

    def from_line(stage, k):
        other, device = peer(*lines[stage], k)
        value = ((), recv_y, recv_z)[stage][other].astype(F32)
        return other, value[:span], value[span:]

    @pl.when(core == lead)
    def _():
        pl.semaphore_wait(barrier, nx - 1 + ny - 1 + ntp - 1 + z)
        for k in reversed(near_first(nx)):
            to_row(k).start()

        @pl.loop(0, z)
        def _(d):
            pl.semaphore_signal(
                ready, inc=1, device_id=(peer(*lines[2], d - z + nz)[1], lead), device_id_type=MESH)

    @pl.when(core != lead)
    def _():
        pl.semaphore_wait(barrier, nx - 1 + ntp - 1)
        for k in list(reversed(near_first(nx))) + [0]:
            to_row(k).start()

    out_par.start()
    for i, s in enumerate(weights):
        pltpu.make_async_copy(s, w_v.at[i, place_of(core)], s_w).start()

    mats_v[...] = jnp.zeros_like(mats_v)
    keep_v[...] = jnp.zeros_like(keep_v)
    settle(c_v, s_c)
    settle(sk_v, s_skip)
    settle(bias_v, s_bias)

    def place(ref, b, l, v_r, v_i):
        at, cols = l * size, l // per * 128
        ref[b, at:at + size, cols:cols + 128] = v_r.astype(BF16)
        ref[b, at:at + size, lanes + cols:lanes + cols + 128] = (-v_i).astype(BF16)

    for g in range(groups):
        b, l = g // gpb, g % gpb
        f_r, f_i = row(1, b)
        cols = slice(l // per * 128, l // per * 128 + 128)
        c_r, c_i = cmul(spread(c_v[0, g], g), spread(c_v[1, g], g), f_r[:, cols], f_i[:, cols])
        gain_v[core, 0, g], gain_v[core, 1, g] = c_r, c_i
        place(mats_v, b, l, c_r, c_i)
    out_gain.start()
    for c in out_w[0]:
        c.start()

    @pl.when(core == lead)
    def _():
        for c in out_w[1]:
            c.start()

    r0, r1 = iota((rows, rows), 0), iota((rows, rows), 1)
    shuffle = jnp.where(r1 == (r0 % chunks) * length + r0 // chunks, 1.0, 0.0).astype(BF16)
    back = jnp.where(r1 == (r0 % length) * chunks + r0 // length, 1.0, 0.0).astype(BF16)
    xp_v[...] = jnp.dot(shuffle, x_v[...], preferred_element_type=F32).astype(BF16)
    crow = iota((chunks, lanes), 0)

    def shift(value, s):
        return jnp.where(crow >= s, pltpu.roll(value, s, 0), 0.0)

    def respond(b):
        out = jnp.dot(xp_v[:, b * 128:(b + 1) * 128], bmat_v[b, 128:], preferred_element_type=F32)
        zr_v[b] = out[:, :lanes]
        zi_v[b] = out[:, lanes:]
        a_r, a_i = power(1, b)
        z_r, z_i = zr_v[b, :chunks, :], zi_v[b, :chunks, :]
        for o in range(1, length):
            here = pl.ds(o * chunks, chunks)
            p_r, p_i = cmul(a_r, a_i, z_r, z_i)
            z_r, z_i = p_r + zr_v[b, here, :], p_i + zi_v[b, here, :]
            zr_v[b, here, :] = z_r
            zi_v[b, here, :] = z_i
        s = 1
        while s < chunks:
            m_r, m_i = cmul(*power(length * s, b), shift(z_r, s), shift(z_i, s))
            z_r, z_i = z_r + m_r, z_i + m_i
            s *= 2
        w_r, w_i = shift(z_r, 1), shift(z_i, 1)
        for o in range(length):
            here = pl.ds(o * chunks, chunks)
            w_r, w_i = cmul(a_r, a_i, w_r, w_i)
            zcat_v[b, here, :lanes] = (zr_v[b, here, :] + w_r).astype(BF16)
            zcat_v[b, here, lanes:] = (zi_v[b, here, :] + w_i).astype(BF16)
        col = pl.ds(b * 128, 128)
        out = nt_dot(zcat_v[b], mats_v[b])
        high = out.astype(BF16)
        low = (out - high.astype(F32)).astype(BF16)
        turned = jnp.dot(back, jnp.concatenate([high, low], axis=1), preferred_element_type=F32)
        resp_v[:, col] = turned[:, :128] + turned[:, 128:] + sk_v[:, col] * x_v[:, col].astype(F32)

    def carry_powers(i, which):
        each = [(b, power(8, b, i)) for b in which]
        value = [cmul(*power(1, b, i), *eight(b, False, i)) for b in which]
        for o in range(half // 16):
            here = pl.ds(o * 16, 16)
            after = [cmul(*e, *v) for (_, e), v in zip(each, value)]
            for (b, _), v, n in zip(each, value, after):
                wcat_v[i, b, here, :lanes] = jnp.concatenate([v[0], n[0]], axis=0).astype(BF16)
                wcat_v[i, b, here, lanes:] = jnp.concatenate([v[1], n[1]], axis=0).astype(BF16)
            value = [cmul(*e, *n) for (_, e), n in zip(each, after)]

    def powers(tab, count, a_r, a_i):
        p_r, p_i = jnp.ones((span, wide), F32), jnp.zeros((span, wide), F32)
        for i in range(count):
            tab[i] = jnp.zeros((2 * span, wide), F32)
            tab[count + i, :span], tab[count + i, span:] = p_r, p_i
            p_r, p_i = cmul(p_r, p_i, a_r, a_i)
        return p_r, p_i

    def weight(tab, at, v_r, v_i):
        return cmul(tab[at, :span], tab[at, span:], v_r, v_i)

    def collect(stage, tab, own_r, own_i, receive):
        at, count, _ = lines[stage]
        t_r, t_i = weight(tab, count + count - 1 - at, own_r, own_i)
        p_r = p_i = jnp.zeros((span, wide), F32)
        for k in near_first(count):
            other, v_r, v_i = receive(k)
            m_r, m_i = weight(tab, count + count - 1 - other, v_r, v_i)
            t_r, t_i = t_r + m_r, t_i + m_i
            m_r, m_i = weight(tab, count + at - 1 - other, v_r, v_i)
            p_r, p_i = p_r + m_r, p_i + m_i
        return t_r, t_i, p_r, p_i

    respond(0)
    got_par.wait_recv()

    @pl.when(core == lead)
    def _():
        ax_r, ax_i = powers(tab_x, nx, *pair(1 + squares))
        ay_r, ay_i = powers(tab_y, ny, ax_r, ax_i)
        sum_v[4], sum_v[5] = ay_r, ay_i
        settle(recv_x.at[pl.ds(0, nx * ntp - 1)], g_x)
        _, own_r, own_i = from_row(0)
        t_r, t_i, p_r, p_i = collect(0, tab_x, own_r, own_i, from_row)
        row_v[:span], row_v[span:] = t_r.astype(BF16), t_i.astype(BF16)
        for k in reversed(near_first(ny)):
            along(1, k).start()
        sum_v[0], sum_v[1], sum_v[2], sum_v[3] = t_r, t_i, p_r, p_i

    for b in range(1, blocks - 1):
        respond(b)
    for b in range(0, blocks, 2):
        carry_powers(core, (b, b + 1))

    respond(blocks - 1)
    out_resp.start()

    @pl.when(core != lead)
    def _():
        for c in out_w[1]:
            c.start()

    both_v[core] = resp_v[rows_of(core), :]
    for b in range(0, blocks, 2):
        carry_powers(other_core, (b, b + 1))

    def hand_on(h_r, h_i):
        pass_v[:span], pass_v[span:] = h_r, h_i
        out_h.start()
        h_v[:span], h_v[span:] = cmul(*pair(late), h_r, h_i)

    @pl.when(core == lead)
    def _():
        s_r, s_i = weight(tab_x, nx + x, tab_y[ny + y, :span], tab_y[ny + y, span:])
        for i in range(nz - 1):
            tab_z[i, :span], tab_z[i, span:] = s_r, s_i
            s_r, s_i = cmul(s_r, s_i, sum_v[4], sum_v[5])
        settle(recv_y.at[pl.ds(0, ny - 1)], g_y)
        t_r, t_i, y_r, y_i = collect(1, tab_y, sum_v[0], sum_v[1], functools.partial(from_line, 1))
        plane_v[:span], plane_v[span:] = t_r.astype(BF16), t_i.astype(BF16)

        @pl.when(z < nz - 1)
        def _():
            pl.semaphore_wait(ready, nz - 1 - z)

        @pl.loop(0, nz - 1 - z)
        def _(i):
            d = jnp.where(z >= nz // 2, nz - 1 - i, z + 1 + i)
            along(2, d - z).start()

        m_r, m_i = weight(tab_x, nx + x, y_r, y_i)
        h_r, h_i = sum_v[2] + m_r, sum_v[3] + m_i
        sum_v[2], sum_v[3] = h_r, h_i

        @pl.when(z == 0)
        def _():
            hand_on(h_r, h_i)

        @pl.when(z > 0)
        def _():
            settle_some(recv_z, g_z, z, nz)

            def gather(k, carry):
                h_r, h_i = carry
                _, v_r, v_i = from_line(2, nz - 1 - k)
                m_r, m_i = weight(tab_z, k, v_r, v_i)
                return h_r + m_r, h_i + m_i

            hand_on(*lax.fori_loop(0, z, gather, (sum_v[2], sum_v[3])))

    @pl.when(core != lead)
    def _():
        out_h.wait_recv()

    got_gain.wait_recv()
    got_resp.wait_recv()
    for i in range(ntp):
        for b in range(blocks):
            for l in range(gpb):
                g, flat = b * gpb + l, l // per * 128
                r, cols = i * tall + b * fold + flat // wide, slice(flat % wide, flat % wide + 128)
                place(keep_v.at[i], b, l, *cmul(
                    gain_v[i, 0, g], gain_v[i, 1, g], h_v[r:r + 1, cols], h_v[span + r:span + r + 1, cols]))
            col = pl.ds(b * 128, 128)
            total = nt_dot(wcat_v[i, b], keep_v[i, b]) + both_v[i, :, col]
            act_v[:, pl.ds(i * depth + b * 128, 128)] = jax.nn.gelu(total).astype(BF16)
    settle(w_v.at[:, place_of(core)], s_w)
    settle(w_v.at[:, place_of(other_core)], g_w)
    piece = min(512, width)
    for j in range(width // piece):
        col = pl.ds(j * piece, piece)
        sums = [bias_v[i, :, col] + jnp.dot(act_v[...], w_v[i, :, col], preferred_element_type=F32) for i in range(2)]
        out_ref[:, col] = (sums[0] * jax.nn.sigmoid(sums[1])).astype(BF16)
    settle(w_v.at[:, place_of(core)], s_c)
    for c in (out_par, out_gain, out_resp):
        c.wait_send()

    @pl.when(core == lead)
    def _():
        settle(recv_x.at[pl.ds(0, nx - 1)], s_step)
        out_h.wait_send()
        settle(recv_y.at[pl.ds(0, ny - 1)], s_x)
        settle_some(recv_z, s_skip, nz - 1 - z, nz)

    @pl.when(core != lead)
    def _():
        settle(recv_x.at[pl.ds(0, nx)], s_step)


def local(nsp, ntp, features, lambda_real, lambda_imag, log_step, input_real, input_imag, real_output,
          imaginary_output, skip_gain, value_weight, gate_weight, value_bias, gate_bias):
    rows, channels = features.shape
    groups, state = lambda_real.shape
    size = input_real.shape[2]
    input_real, input_imag = jnp.swapaxes(input_real, 1, 2), jnp.swapaxes(input_imag, 1, 2)
    width = value_weight.shape[1]
    gpb = 128 // size
    lanes, blocks = gpb * state, groups // gpb
    ring = nz, ny, nx = split_ring(nsp)
    held = (16, 2 * blocks * lanes // 16)
    pairs = (ntp * held[0], held[1])
    half = rows // ntp
    args = (features, lambda_real, lambda_imag, log_step[None], input_real, input_imag, real_output,
            imaginary_output, skip_gain[None], value_weight, gate_weight, value_bias[None], gate_bias[None])
    scratch = [
        pltpu.VMEM(features.shape, BF16),
        pltpu.VMEM((1, groups), F32),
        pltpu.VMEM((2, groups, state), F32),
        pltpu.VMEM((2, groups, size, state), F32),
        pltpu.VMEM((2, groups, size, state), F32),
        pltpu.VMEM((1, channels), F32),
        pltpu.VMEM((2, 1, width), F32),
    ]
    scratch += [
        pltpu.VMEM((2, ntp * channels, width), BF16),
        pltpu.VMEM((rows, channels), BF16),
        pltpu.VMEM((blocks, 256, 2 * lanes), BF16),
        pltpu.VMEM((blocks, 128, 2 * lanes), BF16),
        pltpu.VMEM((ntp, blocks, 128, 2 * lanes), BF16),
        pltpu.VMEM((blocks, rows, lanes), F32),
        pltpu.VMEM((blocks, rows, lanes), F32),
        pltpu.VMEM((blocks, rows, 2 * lanes), BF16),
        pltpu.VMEM((ntp, blocks, half, 2 * lanes), BF16),
        pltpu.VMEM((ntp, 2, groups, size, 128), F32),
        pltpu.VMEM((rows, channels), F32),
        pltpu.VMEM((ntp, half, channels), F32),
        pltpu.VMEM((half, ntp * channels), BF16),
        pltpu.VMEM((ntp, 4 + 2 * (rows.bit_length() - 1), 8, held[1]), F32),
        pltpu.VMEM(held, F32),
        pltpu.VMEM((2 * nx,) + pairs, F32),
        pltpu.VMEM((2 * ny,) + pairs, F32),
        pltpu.VMEM((nz - 1,) + pairs, F32),
        pltpu.VMEM((6, pairs[0] // 2, pairs[1]), F32),
        pltpu.VMEM(held, BF16),
        pltpu.VMEM(pairs, BF16),
        pltpu.VMEM(pairs, BF16),
        pltpu.VMEM((nx * ntp,) + held, BF16),
        pltpu.VMEM((ny,) + pairs, BF16),
        pltpu.VMEM((nz,) + pairs, BF16),
        pltpu.VMEM(pairs, F32),
        pltpu.VMEM(pairs, F32),
        pltpu.SemaphoreType.DMA((9,)),
        pltpu.SemaphoreType.DMA((8,)),
        pltpu.SemaphoreType.REGULAR,
    ]
    return pl.pallas_call(
        functools.partial(kernel, ring, ntp, (rows, groups, state, size, width)),
        out_shape=pltpu.VMEM((rows // ntp, width), BF16),
        in_specs=[pl.BlockSpec(memory_space=pl.ANY)] * len(args),
        out_specs=pl.BlockSpec(memory_space=pltpu.VMEM),
        scratch_shapes=scratch,
        compiler_params=pltpu.CompilerParams(
            collective_id=0, has_side_effects=True, vmem_limit_bytes=60 * 1024 * 1024),
        name="mixer",
    )(*args)


def solution(mesh):
    in_specs = (
        P("sp", "tp"),
        P("tp", None),
        P("tp", None),
        P("tp"),
        P("tp", None, None),
        P("tp", None, None),
        P("tp", None, None),
        P("tp", None, None),
        P("tp"),
        P("tp", None),
        P("tp", None),
        P(),
        P(),
    )
    out_specs = P(("sp", "tp"), None)
    body = functools.partial(local, mesh.shape["sp"], mesh.shape["tp"])
    return jax.shard_map(body, mesh=mesh, in_specs=in_specs, out_specs=out_specs, check_vma=False)
```
